512 devices in a mesh: sp: 64 (over z, y), tp: 8 (over x, core).
Axes of the slice: x: 4, y: 8, z: 8, core: 2. Of those that a mesh axis runs over, the one named last changes fastest.
Arguments:
- tokens: bfloat16 [16384, 1024], P(('sp', 'tp')), may hold values from -16 to 16, as said below
- valid_len: int32 [1], replicated, may hold values from 12288 to 16384
- norm_gain: float32 [1024], replicated, may hold values from 0.5 to 1.5
- w_query: bfloat16 [1024, 4096], P(None, 'tp'), may hold values from -0.1875 to 0.1875
- w_key: bfloat16 [1024, 1024], P(None, 'tp'), may hold values from -0.1875 to 0.1875
- w_value: bfloat16 [1024, 1024], P(None, 'tp'), may hold values from -0.1875 to 0.1875
- q_gain: float32 [128], replicated, may hold values from 0.5 to 1.5
- k_gain: float32 [128], replicated, may hold values from 0.5 to 1.5
- w_out: bfloat16 [4096, 1024], P('tp'), may hold values from -0.375 to 0.375
Outputs:
- mixed: bfloat16 [16384, 1024], P(('sp', 'tp'))
The draws below stay inside these ranges and needn't reach their ends.
Inputs may be any that keep to these rules, and one draw needn't show every extreme that they name: tokens are random entries of unit-order spread (normal or uniform) plus a shift shared by every run of 256 consecutive rows, within -16 and 16. valid_len is at least three quarters of 16384 and at most 16384.
All inputs are finite; a program needn't handle non-finite values.
Results may differ from the reference program's by a relative error of at most 0.02.
Values may be sent and summed in bfloat16 or wider, within the bound.
A program may use at most 64 MiB of HBM per device.

```python
import jax
import jax.numpy as jnp
from jax import lax

D = 1024
HEAD_DIM = 128
KV_HEADS = 8
Q_PER_KV = 4
GRID_W = 64
TOK_DEV = 256
Q_HEADS = 32
TOKENS = 16384
N_SP = 64


def draw_tokens(key, part):
    noise_key = jax.random.fold_in(key, 11)
    shift_key = jax.random.fold_in(key, 12)
    groups = TOKENS // TOK_DEV
    noise_part = jax.random.normal(noise_key, (TOKENS, D), jnp.float32)
    shifts = 1.5 * jax.random.normal(shift_key, (groups, D), jnp.float32)
    shifted = noise_part + jnp.repeat(shifts, TOK_DEV, axis=0)
    return jnp.clip(shifted, -16.0, 16.0).astype(jnp.bfloat16)


def levels(rng, extent, cuts, low, top_value):
    def one(axis_at, parts):
        draws = jax.random.uniform(jax.random.fold_in(jax.random.fold_in(rng, 6), axis_at), (parts,), jnp.float32, low / len(cuts), top_value / len(cuts))
        return jnp.repeat(jnp.exp(draws), extent[axis_at] // parts).reshape((-1,) + (1,) * (len(extent) - axis_at - 1))

    level = one(*cuts[0])
    for cut in cuts[1:]:
        level = level * one(*cut)
    return level


def scatter_about(rng, dims, spread, limit, cuts=(), kind=jnp.bfloat16):
    level = levels(rng, dims, cuts, -0.22, 0.18) if cuts else 1.0
    drawn = jax.random.normal(rng, dims, jnp.float32) * spread * level
    return jnp.minimum(jnp.maximum(drawn, -limit), limit).astype(kind)


def setup_inputs(seed: int = 0) -> dict:
    seeds = jax.random.split(jax.random.key(seed), 10)
    tokens = draw_tokens(jax.random.fold_in(seeds[9], 71), 0)
    valid_len = jax.random.randint(seeds[1], (1,), TOKENS * 3 // 4, TOKENS + 1).astype(jnp.int32)
    norm_gain = jnp.clip(1.0 + 0.1 * jax.random.normal(seeds[2], (D,), jnp.float32), 0.5, 1.5)
    w_query = scatter_about(seeds[3], (D, Q_HEADS * HEAD_DIM), D ** -0.5, 0.1875, ((1, 8),))
    w_key = scatter_about(seeds[4], (D, KV_HEADS * HEAD_DIM), D ** -0.5, 0.1875, ((1, 8),))
    w_value = scatter_about(seeds[5], (D, KV_HEADS * HEAD_DIM), D ** -0.5, 0.1875, ((1, 8),))
    q_gain = jnp.clip(1.0 + 0.1 * jax.random.normal(seeds[6], (HEAD_DIM,), jnp.float32), 0.5, 1.5)
    k_gain = jnp.clip(1.0 + 0.1 * jax.random.normal(seeds[7], (HEAD_DIM,), jnp.float32), 0.5, 1.5)
    w_out = scatter_about(seeds[8], (Q_HEADS * HEAD_DIM, D), (Q_HEADS * HEAD_DIM // 16) ** -0.5, 0.375, ((0, 8),))
    return dict(tokens=tokens, valid_len=valid_len, norm_gain=norm_gain, w_query=w_query, w_key=w_key, w_value=w_value, q_gain=q_gain, k_gain=k_gain, w_out=w_out)


norm_eps = 1e-06
rope_base = 10000.0

def normalize(values, gain):
    scaled = values.astype(jnp.float32)
    return scaled * lax.rsqrt(lax.optimization_barrier(jnp.mean(scaled * scaled, axis=-1, keepdims=True)) + norm_eps) * gain

def rope_tables(positions, head_width):
    quarter = head_width // 4
    half_width = head_width // 2
    frequency = rope_base ** (-(jnp.arange(quarter, dtype=jnp.float32) * 2.0) / half_width)
    grid_row = (positions // GRID_W).astype(jnp.float32)
    grid_col = (positions % GRID_W).astype(jnp.float32)
    row_angle = grid_row[:, None] * frequency[None, :]
    col_angle = grid_col[:, None] * frequency[None, :]
    angles = jnp.concatenate([row_angle, row_angle, col_angle, col_angle], axis=-1)
    return (jnp.cos(angles), jnp.sin(angles))

def turn_half(values):
    width = values.shape[-1] // 2
    return jnp.concatenate([-values[..., width:], values[..., :width]], axis=-1)

def prepare(projected, gain, positions, factor):
    head_width = gain.shape[0]
    shaped = projected.astype(jnp.float32).reshape(projected.shape[0], -1, head_width)
    unit = normalize(shaped, gain)
    half_width = head_width // 2
    turned = jnp.concatenate([turn_half(unit[..., :half_width]), turn_half(unit[..., half_width:])], axis=-1)
    cosine, sine_table = rope_tables(positions, head_width)
    result = unit * cosine[:, None, :] + turned * sine_table[:, None, :]
    return (result * factor).astype(jnp.bfloat16)

def reference(tokens, valid_len, norm_gain, w_query, w_key, w_value, q_gain, k_gain, w_out):
    normed = normalize(tokens, norm_gain).astype(jnp.bfloat16)
    queries = jnp.dot(normed, w_query, preferred_element_type=jnp.float32).astype(jnp.bfloat16)
    keys_all = jnp.dot(normed, w_key, preferred_element_type=jnp.float32).astype(jnp.bfloat16)
    values = jnp.dot(normed, w_value, preferred_element_type=jnp.float32).astype(jnp.bfloat16)
    positions = jnp.arange(TOKENS, dtype=jnp.int32)
    turned_query = lax.optimization_barrier(prepare(queries, q_gain, positions, HEAD_DIM ** (-0.5)))
    turned_key = lax.optimization_barrier(prepare(keys_all, k_gain, positions, 1.0))
    key_wide = turned_key.astype(jnp.float32)
    value_wide = values.reshape(TOKENS, KV_HEADS, HEAD_DIM).astype(jnp.float32)
    key_valid = positions < valid_len[0]
    grouped = turned_query.reshape(N_SP, TOK_DEV, KV_HEADS, Q_PER_KV, HEAD_DIM)

    def attend(query_block):
        scores = jnp.einsum('qgrd,kgd->grqk', query_block.astype(jnp.float32), key_wide)
        scores = jnp.where(key_valid[None, None, None, :], scores, -jnp.inf)
        top = lax.optimization_barrier(jnp.max(scores, axis=-1, keepdims=True))
        weights = jnp.exp(scores - top)
        totals = lax.optimization_barrier(jnp.sum(weights, axis=-1))
        rounded = lax.optimization_barrier(weights.astype(jnp.bfloat16))
        summed = jnp.einsum('grqk,kgd->grqd', rounded.astype(jnp.float32), value_wide)
        result = summed / totals[..., None]
        return result.transpose(2, 0, 1, 3).reshape(TOK_DEV, Q_HEADS * HEAD_DIM).astype(jnp.bfloat16)
    attended = lax.map(attend, grouped).reshape(TOKENS, Q_HEADS * HEAD_DIM)
    return jnp.dot(attended, w_out, preferred_element_type=jnp.float32).astype(jnp.bfloat16)
```

```python
import functools
import math

import jax
import jax.numpy as jnp
import numpy as np
from jax import lax
from jax.experimental import pallas as pl
from jax.experimental.pallas import tpu as pltpu
from jax.sharding import PartitionSpec as P

HEAD_DIM = 128
Q_PER_KV = 4
GRID_W = 64
RING = 8
N_TP = 8
ROWS = 32
BLOCK = 256
HALF = 128
EPS = 1e-06
MESH = pl.DeviceIdType.MESH
OFFSETS = (0, -1, 1, -2, 2, -3, 3, -4)
Q_SCALE = HEAD_DIM ** -0.5 * math.log2(math.e)


def rope_constants():
    freq = np.float32(10000.0) ** (-(np.arange(32, dtype=np.float32) * 2.0) / 64)
    freq = freq.astype(np.float32)
    sign = np.concatenate([-np.ones(32), np.ones(32)]).astype(np.float32)

    def table(count):
        angle = (np.arange(count, dtype=np.float32)[:, None] * freq[None, :]).astype(np.float64)
        angle = np.concatenate([angle, angle], axis=1)
        return np.cos(angle).astype(np.float32), np.sin(angle).astype(np.float32) * sign

    row_cos, row_sin = table(256)
    col_cos, col_sin = table(64)
    rows = np.zeros((64, 8, 128), np.float32)
    rows[:, 0:4, 0:64] = row_cos.reshape(64, 4, 64)
    rows[:, 4:8, 0:64] = row_sin.reshape(64, 4, 64)
    cols = np.zeros((2, 64, 128), np.float32)
    cols[0, :, 64:] = col_cos
    cols[1, :, 64:] = col_sin
    return rows, cols


def kernel(tok, valid, ngain, wq_hbm, wk_hbm, wv_hbm, qgain, kgain, wo_hbm, rowtab_hbm, coltab,
           out, x, wq, wk, wv, wo, rowtab, cosv, sinv, kv, qs, mask, acc, lsum, att, part, rs,
           w_sem, xs_sem, xr_sem, s1_sem, r1_sem, s2_sem, r2_sem, os_sem, or_sem):
    sp = lax.axis_index("sp")
    tp = lax.axis_index("tp")
    z = sp // RING
    y = sp % RING

    def wrap(a):
        return lax.rem(a + 2 * RING, RING)

    def at(zz, yy):
        return {"sp": zz * RING + yy, "tp": tp}

    up = {"y": (at(z, wrap(y + 1)), at(z, wrap(y - 1))), "z": (at(wrap(z + 1), y), at(wrap(z - 1), y))}
    first = ("y", "z")
    second = ("z", "y")
    peers = [{"sp": sp, "tp": lax.rem(tp + k, N_TP)} for k in range(1, N_TP)]

    loads = [
        pltpu.make_async_copy(wk_hbm, wk, w_sem.at[0]),
        pltpu.make_async_copy(wv_hbm, wv, w_sem.at[1]),
        pltpu.make_async_copy(rowtab_hbm.at[sp], rowtab, w_sem.at[2]),
        pltpu.make_async_copy(wq_hbm, wq, w_sem.at[3]),
        pltpu.make_async_copy(wo_hbm, wo, w_sem.at[4]),
    ]
    for load in loads:
        load.start()

    barrier = pltpu.get_barrier_semaphore()
    everyone = peers + [up["y"][0], up["y"][1], up["z"][0], up["z"][1]]
    for peer in everyone:
        pl.semaphore_signal(barrier, inc=1, device_id=peer, device_id_type=MESH)

    scaled = tok[...].astype(jnp.float32)
    inv = lax.rsqrt(jnp.mean(scaled * scaled, axis=-1, keepdims=True) + EPS)
    x[tp] = (scaled * inv * ngain[...]).astype(jnp.bfloat16)
    acc[...] = jnp.zeros_like(acc)
    lsum[...] = jnp.zeros_like(lsum)

    pl.semaphore_wait(barrier, len(everyone))

    def xcopy(k):
        return pltpu.make_async_remote_copy(
            src_ref=x.at[tp], dst_ref=x.at[tp], send_sem=xs_sem.at[k], recv_sem=xr_sem.at[k],
            device_id=peers[k], device_id_type=MESH)

    for k in range(N_TP - 1):
        xcopy(k).start()

    loads[2].wait()
    for r in range(4):
        cosv[r * 64:(r + 1) * 64, :] = rowtab[r:r + 1, :] + coltab[0]
        sinv[r * 64:(r + 1) * 64, :] = rowtab[4 + r:5 + r, :] + coltab[1]

    limit = valid[0]
    lane = lax.broadcasted_iota(jnp.int32, (1, HALF), 1)

    def mask_row(slot, block, half):
        pos = block * BLOCK + half * HALF + lane
        mask[slot] = jnp.broadcast_to((pos < limit).astype(jnp.float32), (8, HALF))

    for part_id in range(2):
        for p in range(8):
            def source(dist, p=p, part_id=part_id):
                if part_id == 0:
                    return wrap(z + dist) * RING + wrap(y + OFFSETS[p])
                return wrap(z + OFFSETS[p]) * RING + wrap(y + dist)
            mask_row(part_id * 64 + p, source(0), part_id)
            sub, q = p // 4, p % 4
            for dist in range(1, 4):
                j = (dist - 1) * 2 + sub
                mask_row(part_id * 64 + 8 + 4 * j + q, source(-dist), part_id)
                mask_row(part_id * 64 + 36 + 4 * j + q, source(dist), part_id)
            mask_row(part_id * 64 + (8 if sub == 0 else 36) + 24 + q, source(-4), part_id)

    loads[0].wait()
    loads[1].wait()
    for k in range(N_TP - 1):
        xcopy(k).wait_recv()

    everything = x[...].reshape(BLOCK, x.shape[2])
    cosine = cosv[...]
    sine = sinv[...]
    in_first = (lax.broadcasted_iota(jnp.int32, (BLOCK, HEAD_DIM), 1) % 64) < 32

    def turn(projected, gain, factor):
        v = projected.astype(jnp.bfloat16).astype(jnp.float32)
        u = v * lax.rsqrt(jnp.mean(v * v, axis=-1, keepdims=True) + EPS) * gain
        moved = jnp.where(in_first, pltpu.roll(u, 96, 1), pltpu.roll(u, 32, 1))
        return (u * cosine + moved * sine) * factor

    keys = turn(jnp.dot(everything, wk[...], preferred_element_type=jnp.float32), kgain[...], 1.0)
    rows = sp * BLOCK + lax.broadcasted_iota(jnp.int32, (BLOCK, HEAD_DIM), 0)
    vals = jnp.dot(everything, wv[...], preferred_element_type=jnp.float32)
    vals = jnp.where(rows < limit, vals, 0.0).astype(jnp.bfloat16)
    for part_id in range(2):
        piece = slice(part_id * HALF, (part_id + 1) * HALF)
        kv[part_id * 64, 0:HALF, :] = keys[piece, :].T.astype(jnp.bfloat16)
        kv[part_id * 64, HALF:, :] = vals[piece, :]

    def hop(part_id, h, d):
        if d == 0:
            src, dst = (0 if h == 1 else 2 * h - 3), 2 * h - 1
        else:
            src, dst = (0 if h == 1 else 2 * h - 2), 2 * h
        return pltpu.make_async_remote_copy(
            src_ref=kv.at[part_id * 64 + src], dst_ref=kv.at[part_id * 64 + dst],
            send_sem=s1_sem.at[part_id, d, h - 1], recv_sem=r1_sem.at[part_id, d, h - 1],
            device_id=up[first[part_id]][d], device_id_type=MESH)

    def place(part_id, d, j):
        return part_id * 64 + 8 + 28 * d + 4 * j

    def hand_on(part_id, d, p):
        return pltpu.make_async_remote_copy(
            src_ref=kv.at[part_id * 64 + p], dst_ref=kv.at[place(part_id, d, p // 4) + p % 4],
            send_sem=s2_sem.at[part_id, d, p // 4], recv_sem=r2_sem.at[part_id, d, p // 4],
            device_id=up[second[part_id]][d], device_id_type=MESH)

    def relay(part_id, d, j, to):
        return pltpu.make_async_remote_copy(
            src_ref=kv.at[pl.ds(place(part_id, d, j), 4)], dst_ref=kv.at[pl.ds(place(part_id, d, to), 4)],
            send_sem=s2_sem.at[part_id, d, to], recv_sem=r2_sem.at[part_id, d, to],
            device_id=up[second[part_id]][d], device_id_type=MESH)

    both = [(a, d) for a in range(2) for d in range(2)]
    for a, d in both:
        hop(a, 1, d).start()
    for a, d in both:
        hand_on(a, d, 0).start()

    loads[3].wait()
    for h in range(Q_PER_KV):
        query = jnp.dot(everything, wq[:, h * HEAD_DIM:(h + 1) * HEAD_DIM], preferred_element_type=jnp.float32)
        qs[h * BLOCK:(h + 1) * BLOCK, :] = turn(query, qgain[...], Q_SCALE).astype(jnp.bfloat16)

    def attend(base0, base1):
        slots = [base0 + i for i in range(4)] + [base1 + i for i in range(4)]
        kt = jnp.concatenate([kv[s, 0:HALF, :] for s in slots], axis=1)
        v = jnp.concatenate([kv[s, HALF:, :] for s in slots], axis=0)
        marks = [mask[s, 0:1, :] for s in slots]
        for r in range(2):
            span = pl.ds(r * 512, 512)
            s = jnp.dot(qs[span, :], kt, preferred_element_type=jnp.float32)
            w = jnp.exp2(s)
            acc[span, :] += jnp.dot(w.astype(jnp.bfloat16), v, preferred_element_type=jnp.float32)
            t = w[:, 0:HALF] * marks[0]
            for i in range(1, 8):
                t = t + w[:, i * HALF:(i + 1) * HALF] * marks[i]
            lsum[span, :] += t

    def first_step(h):
        ways = (0, 1) if h < 4 else (0,)
        for a in range(2):
            for d in ways:
                hop(a, h, d).wait_recv()
                if h + 1 < 4 or (h + 1 == 4 and d == 0):
                    hop(a, h + 1, d).start()
        for a in range(2):
            for d in ways:
                for e in range(2):
                    hand_on(a, e, 2 * h - 1 + d).start()

    for h in (1, 2, 3):
        first_step(h)
    for a, d in both:
        relay(a, d, 0, 0).wait_recv()
        relay(a, d, 0, 2).start()
    first_step(4)

    def own(a, c):
        attend(a * 64, a * 64 + 4)
        return c

    lax.fori_loop(0, 2, own, 0)

    def step(j, c):
        for a in range(2):
            for d in range(2):
                @pl.when(j > 0)
                def _():
                    relay(a, d, j, j).wait_recv()

                    @pl.when(j < (5 if d == 0 else 4))
                    def _():
                        relay(a, d, j, j + 2).start()
                    if d == 1:
                        @pl.when(j == 5)
                        def _():
                            relay(a, d, j, j + 1).start()
            attend(place(a, 0, j), place(a, 1, j))
        return c

    lax.fori_loop(0, 7, step, 0)

    loads[4].wait()
    for h in range(Q_PER_KV):
        span = slice(h * BLOCK, (h + 1) * BLOCK)
        total = jnp.sum(lsum[span, :], axis=-1, keepdims=True)
        att[:, h * HEAD_DIM:(h + 1) * HEAD_DIM] = (acc[span, :] / total).astype(jnp.bfloat16)
    mixed = jnp.dot(att[...], wo[...], preferred_element_type=jnp.float32)
    part[...] = mixed.astype(jnp.bfloat16).reshape(part.shape)

    def ocopy(k):
        return pltpu.make_async_remote_copy(
            src_ref=part.at[lax.rem(tp + k + 1, N_TP)], dst_ref=rs.at[k], send_sem=os_sem.at[k],
            recv_sem=or_sem.at[k], device_id=peers[k], device_id_type=MESH)

    for k in range(N_TP - 1):
        ocopy(k).start()

    for k in range(N_TP - 1):
        xcopy(k).wait_send()
    for a, d in both:
        for h in range(1, 5 - d):
            hop(a, h, d).wait_send()
        for j in range(7):
            relay(a, d, 0, j).wait_send()

    total = part[tp].astype(jnp.float32)
    for k in range(N_TP - 1):
        ocopy(k).wait_recv()
        total = total + rs[k].astype(jnp.float32)
    out[...] = total.astype(jnp.bfloat16)
    for k in range(N_TP - 1):
        ocopy(k).wait_send()


def on_device(tokens, valid_len, norm_gain, w_query, w_key, w_value, q_gain, k_gain, w_out):
    rows, cols = rope_constants()
    width = tokens.shape[1]
    vmem = pl.BlockSpec(memory_space=pltpu.VMEM)
    anywhere = pl.BlockSpec(memory_space=pl.ANY)
    dma = pltpu.SemaphoreType.DMA
    call = pl.pallas_call(
        kernel,
        out_shape=jax.ShapeDtypeStruct(tokens.shape, jnp.bfloat16),
        in_specs=[vmem, pl.BlockSpec(memory_space=pltpu.SMEM), vmem, anywhere, anywhere, anywhere,
                  vmem, vmem, anywhere, anywhere, vmem],
        out_specs=vmem,
        scratch_shapes=[
            pltpu.VMEM((N_TP, ROWS, width), jnp.bfloat16),
            pltpu.VMEM(w_query.shape, jnp.bfloat16),
            pltpu.VMEM(w_key.shape, jnp.bfloat16),
            pltpu.VMEM(w_value.shape, jnp.bfloat16),
            pltpu.VMEM(w_out.shape, jnp.bfloat16),
            pltpu.VMEM((8, HEAD_DIM), jnp.float32),
            pltpu.VMEM((BLOCK, HEAD_DIM), jnp.float32),
            pltpu.VMEM((BLOCK, HEAD_DIM), jnp.float32),
            pltpu.VMEM((128, 2 * HALF, HEAD_DIM), jnp.bfloat16),
            pltpu.VMEM((Q_PER_KV * BLOCK, HEAD_DIM), jnp.bfloat16),
            pltpu.VMEM((128, 8, HALF), jnp.float32),
            pltpu.VMEM((Q_PER_KV * BLOCK, HEAD_DIM), jnp.float32),
            pltpu.VMEM((Q_PER_KV * BLOCK, HEAD_DIM), jnp.float32),
            pltpu.VMEM((BLOCK, Q_PER_KV * HEAD_DIM), jnp.bfloat16),
            pltpu.VMEM((N_TP, ROWS, width), jnp.bfloat16),
            pltpu.VMEM((N_TP - 1, ROWS, width), jnp.bfloat16),
            dma((5,)), dma((7,)), dma((7,)), dma((2, 2, 4)), dma((2, 2, 4)), dma((2, 2, 7)), dma((2, 2, 7)),
            dma((7,)), dma((7,)),
        ],
        compiler_params=pltpu.CompilerParams(
            collective_id=0, has_side_effects=True, vmem_limit_bytes=48 * 2 ** 20),
        name="fused_attention",
    )
    return call(tokens, valid_len, norm_gain.reshape(1, -1), w_query, w_key, w_value,
                q_gain.reshape(1, -1), k_gain.reshape(1, -1), w_out, jnp.asarray(rows), jnp.asarray(cols))


def solution(mesh):
    return jax.shard_map(
        on_device,
        mesh=mesh,
        in_specs=(
            P(("sp", "tp"), None),
            P(),
            P(),
            P(None, "tp"),
            P(None, "tp"),
            P(None, "tp"),
            P(),
            P(),
            P("tp", None),
        ),
        out_specs=P(("sp", "tp"), None),
        check_vma=False,
    )
```

```python
import functools
import math

import jax
import jax.numpy as jnp
import numpy as np
from jax import lax
from jax.experimental import pallas as pl
from jax.experimental.pallas import tpu as pltpu
from jax.sharding import PartitionSpec as P

HEAD_DIM = 128
Q_PER_KV = 4
GRID_W = 64
RING = 8
N_TP = 8
N_X = 4
ROWS = 32
BLOCK = 256
HALF = 128
EPS = 1e-06
MESH = pl.DeviceIdType.MESH
OFFSETS = (0, -1, 1, -2, 2, -3, 3, -4)
Q_SCALE = HEAD_DIM ** -0.5 * math.log2(math.e)


def rope_constants():
    freq = np.float32(10000.0) ** (-(np.arange(32, dtype=np.float32) * 2.0) / 64)
    freq = freq.astype(np.float32)
    sign = np.concatenate([-np.ones(32), np.ones(32)]).astype(np.float32)

    def table(count):
        angle = (np.arange(count, dtype=np.float32)[:, None] * freq[None, :]).astype(np.float64)
        angle = np.concatenate([angle, angle], axis=1)
        return np.cos(angle).astype(np.float32), np.sin(angle).astype(np.float32) * sign

    row_cos, row_sin = table(256)
    col_cos, col_sin = table(64)
    rows = np.zeros((64, 8, 128), np.float32)
    rows[:, 0:4, 0:64] = row_cos.reshape(64, 4, 64)
    rows[:, 4:8, 0:64] = row_sin.reshape(64, 4, 64)
    cols = np.zeros((2, 64, 128), np.float32)
    cols[0, :, 64:] = col_cos
    cols[1, :, 64:] = col_sin
    return rows, cols


def kernel(tok_hbm, valid, ngain_hbm, wq_hbm, wk_hbm, wv_hbm, qgain_hbm, kgain_hbm, wo_hbm, rowtab_hbm, coltab_hbm,
           out, tok, ngain, qgain, kgain, coltab, x, wq, wk, wv, wo, rowtab, cosv, sinv, kv, qs, mask, acc, lsum, att, partial, to_twin, from_twin, summed, arrived,
           w_sem, xs_sem, xr_sem, s1_sem, r1_sem, s2_sem, r2_sem, ds_sem, dr_sem, os_sem, or_sem):
    sp = lax.axis_index("sp")
    tp = lax.axis_index("tp")
    z = sp // RING
    y = sp % RING

    def wrap(a):
        return lax.rem(a + 2 * RING, RING)

    def at(zz, yy):
        return {"sp": zz * RING + yy, "tp": tp}

    up = {"y": (at(z, wrap(y + 1)), at(z, wrap(y - 1))), "z": (at(wrap(z + 1), y), at(wrap(z - 1), y))}
    first = ("y", "z")
    second = ("z", "y")
    core = lax.rem(tp, 2)
    column = tp // 2
    twin = {"sp": sp, "tp": tp + 1 - 2 * core}
    peers = [{"sp": sp, "tp": lax.rem(tp + 2 * k, N_TP)} for k in range(1, N_X)]

    loads = [
        pltpu.make_async_copy(wk_hbm, wk, w_sem.at[0]),
        pltpu.make_async_copy(wv_hbm, wv, w_sem.at[1]),
        pltpu.make_async_copy(rowtab_hbm.at[sp], rowtab, w_sem.at[2]),
        pltpu.make_async_copy(wq_hbm, wq, w_sem.at[3]),
        pltpu.make_async_copy(wo_hbm, wo, w_sem.at[4]),
        pltpu.make_async_copy(coltab_hbm, coltab, w_sem.at[5]),
        pltpu.make_async_copy(qgain_hbm, qgain, w_sem.at[6]),
        pltpu.make_async_copy(kgain_hbm, kgain, w_sem.at[7]),
    ]
    early = [
        pltpu.make_async_copy(tok_hbm, tok, w_sem.at[8]),
        pltpu.make_async_copy(ngain_hbm, ngain, w_sem.at[9]),
    ]
    for load in early:
        load.start()
    for load in loads:
        load.start()

    barrier = pltpu.get_barrier_semaphore()
    everyone = peers + [twin, up["y"][0], up["y"][1], up["z"][0], up["z"][1]]
    for peer in everyone:
        pl.semaphore_signal(barrier, inc=1, device_id=peer, device_id_type=MESH)

    for load in early:
        load.wait()
    scaled = tok[...].astype(jnp.float32)
    inv = lax.rsqrt(jnp.mean(scaled * scaled, axis=-1, keepdims=True) + EPS)
    x[tp] = (scaled * inv * ngain[...]).astype(jnp.bfloat16)
    acc[...] = jnp.zeros_like(acc)
    lsum[...] = jnp.zeros_like(lsum)

    pl.semaphore_wait(barrier, len(everyone))

    def xcopy(i):
        slot = tp if i < N_X else lax.rem(tp + 2 * N_TP - 2 * (i - N_X + 1), N_TP)
        return pltpu.make_async_remote_copy(
            src_ref=x.at[slot], dst_ref=x.at[slot], send_sem=xs_sem.at[i], recv_sem=xr_sem.at[i],
            device_id=peers[i - 1] if 0 < i < N_X else twin, device_id_type=MESH)

    for i in (2, 1, 3, 0):
        xcopy(i).start()

    for i in (2, 5, 6, 7):
        loads[i].wait()
    for r in range(4):
        cosv[r * 64:(r + 1) * 64, :] = rowtab[r:r + 1, :] + coltab[0]
        sinv[r * 64:(r + 1) * 64, :] = rowtab[4 + r:5 + r, :] + coltab[1]

    limit = valid[0]
    lane = lax.broadcasted_iota(jnp.int32, (1, HALF), 1)

    def mask_row(slot, block, half):
        pos = block * BLOCK + half * HALF + lane
        mask[slot] = jnp.broadcast_to((pos < limit).astype(jnp.float32), (8, HALF))

    for part_id in range(2):
        for p in range(8):
            def source(dist, p=p, part_id=part_id):
                if part_id == 0:
                    return wrap(z + dist) * RING + wrap(y + OFFSETS[p])
                return wrap(z + OFFSETS[p]) * RING + wrap(y + dist)
            mask_row(part_id * 64 + p, source(0), part_id)
            sub, q = p // 4, p % 4
            for dist in range(1, 4):
                j = (dist - 1) * 2 + sub
                mask_row(part_id * 64 + 8 + 4 * j + q, source(-dist), part_id)
                mask_row(part_id * 64 + 36 + 4 * j + q, source(dist), part_id)
            mask_row(part_id * 64 + (8 if sub == 0 else 36) + 24 + q, source(-4), part_id)

    loads[0].wait()
    loads[1].wait()
    for k in (1, 3, 2):
        xcopy(k).wait_recv()
        xcopy(k + N_X - 1).start()
    for i in (0, 4, 6, 5):
        xcopy(i).wait_recv()

    everything = x[...].reshape(BLOCK, x.shape[2])
    cosine = cosv[...]
    sine = sinv[...]
    in_first = (lax.broadcasted_iota(jnp.int32, (BLOCK, HEAD_DIM), 1) % 64) < 32

    def turn(projected, gain, factor):
        v = projected.astype(jnp.bfloat16).astype(jnp.float32)
        u = v * lax.rsqrt(jnp.mean(v * v, axis=-1, keepdims=True) + EPS) * gain
        moved = jnp.where(in_first, pltpu.roll(u, 96, 1), pltpu.roll(u, 32, 1))
        return (u * cosine + moved * sine) * factor

    keys = turn(jnp.dot(everything, wk[...], preferred_element_type=jnp.float32), kgain[...], 1.0)
    rows = sp * BLOCK + lax.broadcasted_iota(jnp.int32, (BLOCK, HEAD_DIM), 0)
    vals = jnp.dot(everything, wv[...], preferred_element_type=jnp.float32)
    vals = jnp.where(rows < limit, vals, 0.0).astype(jnp.bfloat16)
    for part_id in range(2):
        piece = slice(part_id * HALF, (part_id + 1) * HALF)
        kv[part_id * 64, 0:HALF, :] = keys[piece, :].T.astype(jnp.bfloat16)
        kv[part_id * 64, HALF:, :] = vals[piece, :]

    def hop(part_id, h, d):
        if d == 0:
            src, dst = (0 if h == 1 else 2 * h - 3), 2 * h - 1
        else:
            src, dst = (0 if h == 1 else 2 * h - 2), 2 * h
        return pltpu.make_async_remote_copy(
            src_ref=kv.at[part_id * 64 + src], dst_ref=kv.at[part_id * 64 + dst],
            send_sem=s1_sem.at[part_id, d, h - 1], recv_sem=r1_sem.at[part_id, d, h - 1],
            device_id=up[first[part_id]][d], device_id_type=MESH)

    def place(part_id, d, j):
        return part_id * 64 + 8 + 28 * d + 4 * j

    def hand_on(part_id, d, p):
        return pltpu.make_async_remote_copy(
            src_ref=kv.at[part_id * 64 + p], dst_ref=kv.at[place(part_id, d, p // 4) + p % 4],
            send_sem=s2_sem.at[part_id, d, p // 4], recv_sem=r2_sem.at[part_id, d, p // 4],
            device_id=up[second[part_id]][d], device_id_type=MESH)

    def relay(part_id, d, j, to):
        return pltpu.make_async_remote_copy(
            src_ref=kv.at[pl.ds(place(part_id, d, j), 4)], dst_ref=kv.at[pl.ds(place(part_id, d, to), 4)],
            send_sem=s2_sem.at[part_id, d, to], recv_sem=r2_sem.at[part_id, d, to],
            device_id=up[second[part_id]][d], device_id_type=MESH)

    def last(part_id, d, i):
        return pltpu.make_async_remote_copy(
            src_ref=kv.at[pl.ds(place(part_id, d, 4 + d) + 2 * i, 2)],
            dst_ref=kv.at[pl.ds(place(part_id, d, 6) + 2 * i, 2)],
            send_sem=s2_sem.at[part_id, d, 6 + i], recv_sem=r2_sem.at[part_id, d, 6 + i],
            device_id=up[second[part_id]][d], device_id_type=MESH)

    both = [(a, d) for a in range(2) for d in range(2)]
    for a, d in both:
        hop(a, 1, d).start()
    for a, d in both:
        hand_on(a, d, 0).start()

    loads[3].wait()
    for h in range(Q_PER_KV):
        query = jnp.dot(everything, wq[:, h * HEAD_DIM:(h + 1) * HEAD_DIM], preferred_element_type=jnp.float32)
        query = turn(query, qgain[...], Q_SCALE).astype(jnp.bfloat16)
        for r in range(2):
            qs[r * 512 + h * HALF:r * 512 + (h + 1) * HALF, :] = query[r * HALF:(r + 1) * HALF, :]

    def attend(slots, rows):
        kt = jnp.concatenate([kv[s, 0:HALF, :] for s in slots], axis=1)
        v = jnp.concatenate([kv[s, HALF:, :] for s in slots], axis=0)
        marks = [mask[s, 0:1, :] for s in slots]
        for r in rows:
            span = pl.ds(r * 512, 512)
            s = jnp.dot(qs[span, :], kt, preferred_element_type=jnp.float32)
            w = jnp.exp2(s)
            acc[span, :] += jnp.dot(w.astype(jnp.bfloat16), v, preferred_element_type=jnp.float32)
            t = w[:, 0:HALF] * marks[0]
            for i in range(1, 8):
                t = t + w[:, i * HALF:(i + 1) * HALF] * marks[i]
            lsum[span, :] += t

    def first_step(h):
        ways = (0, 1) if h < 4 else (0,)
        for a in range(2):
            for d in ways:
                hop(a, h, d).wait_recv()
                if h + 1 < 4 or (h + 1 == 4 and d == 0):
                    hop(a, h + 1, d).start()
        for a in range(2):
            for d in ways:
                for e in range(2):
                    hand_on(a, e, 2 * h - 1 + d).start()

    for h in (1, 2, 3, 4):
        first_step(h)
    for a, d in both:
        relay(a, d, 0, 0).wait_recv()
        relay(a, d, 0, 2).start()

    def own(a, c):
        attend([a * 64 + i for i in range(8)], (0, 1))
        return c

    lax.fori_loop(0, 2, own, 0)

    def step(j, c):
        for a in range(2):
            for d in range(2):
                @pl.when(j > 0)
                def _():
                    relay(a, d, j, j).wait_recv()

                    @pl.when(j < 4)
                    def _():
                        relay(a, d, j, j + 2).start()

                    @pl.when(j == 4 + d)
                    def _():
                        last(a, d, 0).start()
                        last(a, d, 1).start()
            attend([place(a, d, j) + i for d in range(2) for i in range(4)], (0, 1))
        return c

    lax.fori_loop(0, 6, step, 0)

    def final_slots(i):
        return [place(a, d, 6) + 2 * i + q for a, d in both for q in range(2)]

    for a, d in both:
        last(a, d, 0).wait_recv()
    attend(final_slots(0), (0, 1))
    for a, d in both:
        last(a, d, 1).wait_recv()

    def project_out(r):
        for h in range(Q_PER_KV):
            span = slice(r * 512 + h * HALF, r * 512 + (h + 1) * HALF)
            total = jnp.sum(lsum[span, :], axis=-1, keepdims=True)
            att[r, :, h * HEAD_DIM:(h + 1) * HEAD_DIM] = (acc[span, :] / total).astype(jnp.bfloat16)
        mixed = jnp.dot(att[r], wo[...], preferred_element_type=jnp.float32)
        partial[4 * r:4 * r + 4] = mixed.reshape(4, ROWS, mixed.shape[1])
        for i in (2 * r, 2 * r + 1):
            to_twin[i] = partial[2 * i + 1 - core].astype(jnp.bfloat16)
            pair(i).start()

    def pair(i):
        return pltpu.make_async_remote_copy(
            src_ref=to_twin.at[i], dst_ref=from_twin.at[i], send_sem=ds_sem.at[i], recv_sem=dr_sem.at[i],
            device_id=twin, device_id_type=MESH)

    def along(i):
        return pltpu.make_async_remote_copy(
            src_ref=summed.at[i], dst_ref=arrived.at[column], send_sem=os_sem.at[i],
            recv_sem=or_sem.at[column], device_id={"sp": sp, "tp": 2 * i + core}, device_id_type=MESH)

    def arrival(source):
        return pltpu.make_async_remote_copy(
            src_ref=summed.at[0], dst_ref=arrived.at[source], send_sem=os_sem.at[0],
            recv_sem=or_sem.at[source], device_id=twin, device_id_type=MESH)

    def add_pair(i):
        pair(i).wait_recv()
        both_cores = partial[2 * i + core] + from_twin[i].astype(jnp.float32)
        partial[2 * i + core] = both_cores
        summed[i] = both_cores.astype(jnp.bfloat16)

        @pl.when(column != i)
        def _():
            along(i).start()

    loads[4].wait()
    attend(final_slots(1), (0,))
    project_out(0)
    attend(final_slots(1), (1,))
    add_pair(0)
    add_pair(1)
    project_out(1)

    for i in range(2 * N_X - 1):
        xcopy(i).wait_send()
    for a, d in both:
        for h in range(1, 5 - d):
            hop(a, h, d).wait_send()
        for j in range(6):
            relay(a, d, 0, j).wait_send()
        for i in range(2):
            last(a, d, i).wait_send()

    add_pair(2)
    add_pair(3)
    total = partial[tp]
    for k in range(1, N_X):
        source = lax.rem(column + N_X - k, N_X)
        arrival(source).wait_recv()
        total = total + arrived[source].astype(jnp.float32)
    out[...] = total.astype(jnp.bfloat16)
    for i in range(N_X):
        pair(i).wait_send()

        @pl.when(column != i)
        def _():
            along(i).wait_send()


def on_device(tokens, valid_len, norm_gain, w_query, w_key, w_value, q_gain, k_gain, w_out):
    rows, cols = rope_constants()
    width = tokens.shape[1]
    vmem = pl.BlockSpec(memory_space=pltpu.VMEM)
    anywhere = pl.BlockSpec(memory_space=pltpu.HBM)
    dma = pltpu.SemaphoreType.DMA
    call = pl.pallas_call(
        kernel,
        out_shape=jax.ShapeDtypeStruct(tokens.shape, jnp.bfloat16),
        in_specs=[anywhere, pl.BlockSpec(memory_space=pltpu.SMEM)] + [anywhere] * 9,
        out_specs=vmem,
        scratch_shapes=[
            pltpu.VMEM(tokens.shape, jnp.bfloat16),
            pltpu.VMEM((1, width), jnp.float32),
            pltpu.VMEM((1, HEAD_DIM), jnp.float32),
            pltpu.VMEM((1, HEAD_DIM), jnp.float32),
            pltpu.VMEM(cols.shape, jnp.float32),
            pltpu.VMEM((N_TP, ROWS, width), jnp.bfloat16),
            pltpu.VMEM(w_query.shape, jnp.bfloat16),
            pltpu.VMEM(w_key.shape, jnp.bfloat16),
            pltpu.VMEM(w_value.shape, jnp.bfloat16),
            pltpu.VMEM(w_out.shape, jnp.bfloat16),
            pltpu.VMEM((8, HEAD_DIM), jnp.float32),
            pltpu.VMEM((BLOCK, HEAD_DIM), jnp.float32),
            pltpu.VMEM((BLOCK, HEAD_DIM), jnp.float32),
            pltpu.VMEM((128, 2 * HALF, HEAD_DIM), jnp.bfloat16),
            pltpu.VMEM((Q_PER_KV * BLOCK, HEAD_DIM), jnp.bfloat16),
            pltpu.VMEM((128, 8, HALF), jnp.float32),
            pltpu.VMEM((Q_PER_KV * BLOCK, HEAD_DIM), jnp.float32),
            pltpu.VMEM((Q_PER_KV * BLOCK, HEAD_DIM), jnp.float32),
            pltpu.VMEM((2, HALF, Q_PER_KV * HEAD_DIM), jnp.bfloat16),
            pltpu.VMEM((N_TP, ROWS, width), jnp.float32),
            pltpu.VMEM((N_X, ROWS, width), jnp.bfloat16),
            pltpu.VMEM((N_X, ROWS, width), jnp.bfloat16),
            pltpu.VMEM((N_X, ROWS, width), jnp.bfloat16),
            pltpu.VMEM((N_X, ROWS, width), jnp.bfloat16),
            dma((10,)), dma((7,)), dma((7,)), dma((2, 2, 4)), dma((2, 2, 4)), dma((2, 2, 8)), dma((2, 2, 8)),
            dma((N_X,)), dma((N_X,)), dma((N_X,)), dma((N_X,)),
        ],
        compiler_params=pltpu.CompilerParams(
            collective_id=0, has_side_effects=True, vmem_limit_bytes=67043328),
        name="fused_attention",
    )
    return call(tokens, valid_len, norm_gain.reshape(1, -1), w_query, w_key, w_value,
                q_gain.reshape(1, -1), k_gain.reshape(1, -1), w_out, jnp.asarray(rows), jnp.asarray(cols))


def solution(mesh):
    return jax.shard_map(
        on_device,
        mesh=mesh,
        in_specs=(
            P(("sp", "tp"), None),
            P(),
            P(),
            P(None, "tp"),
            P(None, "tp"),
            P(None, "tp"),
            P(),
            P(),
            P("tp", None),
        ),
        out_specs=P(("sp", "tp"), None),
        check_vma=False,
    )
```

```python
import functools
import math

import jax
import jax.numpy as jnp
import numpy as np
from jax import lax
from jax.experimental import pallas as pl
from jax.experimental.pallas import tpu as pltpu
from jax.sharding import PartitionSpec as P

HEAD_DIM = 128
Q_PER_KV = 4
GRID_W = 64
RING = 8
N_TP = 8
N_X = 4
ROWS = 32
BLOCK = 256
HALF = 128
EPS = 1e-06
MESH = pl.DeviceIdType.MESH
STAY = (0, 2, -2, 4)
MOVE = (1, -1, 3, -3)
SOURCE = (0, -1, -2, -3, 1, 2, 3, 4)
Q_SCALE = HEAD_DIM ** -0.5 * math.log2(math.e)


def rope_constants():
    freq = np.float32(10000.0) ** (-(np.arange(32, dtype=np.float32) * 2.0) / 64)
    freq = freq.astype(np.float32)
    sign = np.concatenate([-np.ones(32), np.ones(32)]).astype(np.float32)

    def table(count):
        angle = (np.arange(count, dtype=np.float32)[:, None] * freq[None, :]).astype(np.float64)
        angle = np.concatenate([angle, angle], axis=1)
        return np.cos(angle).astype(np.float32), np.sin(angle).astype(np.float32) * sign

    row_cos, row_sin = table(256)
    col_cos, col_sin = table(64)
    rows = np.zeros((64, 8, 128), np.float32)
    rows[:, 0:4, 0:64] = row_cos.reshape(64, 4, 64)
    rows[:, 4:8, 0:64] = row_sin.reshape(64, 4, 64)
    cols = np.zeros((2, 64, 128), np.float32)
    cols[0, :, 64:] = col_cos
    cols[1, :, 64:] = col_sin
    return rows, cols


def kernel(tok_hbm, valid, ngain_hbm, wq_hbm, wk_hbm, wv_hbm, qgain_hbm, kgain_hbm, wo_hbm, rowtab_hbm, coltab_hbm,
           out, tok, ngain, qgain, kgain, coltab, x, wq, wk, wv, wo, rowtab, cosv, sinv, mine, kv, qs, q, mask, acc, lsum, o_out, o_in, l_out, l_in, den, att, partial, to_twin, from_twin, summed, arrived,
           w_sem, xs_sem, xr_sem, s1_sem, r1_sem, s2_sem, r2_sem,
           st_sem, rt_sem, qs_sem, qr_sem, gs_sem, gr_sem, ds_sem, dr_sem, os_sem, or_sem):
    sp = lax.axis_index("sp")
    tp = lax.axis_index("tp")
    z = sp // RING
    y = sp % RING

    def wrap(a):
        return lax.rem(a + 2 * RING, RING)

    core = lax.rem(tp, 2)
    column = tp // 2
    other = tp + 1 - 2 * core
    twin = {"sp": sp, "tp": other}
    peers = [{"sp": sp, "tp": lax.rem(tp + 2 * k, N_TP)} for k in range(1, N_X)]
    moves = (core != lax.rem(y, 2), core != lax.rem(z, 2))
    moved = [m.astype(jnp.int32) for m in moves]

    def at(part_id, first, second, where):
        dz, dy = (second, first) if part_id == 0 else (first, second)
        return {"sp": wrap(z + dz) * RING + wrap(y + dy), "tp": where}

    ring = [[at(a, 0, step, tp) for step in (1, -1)] for a in range(2)]
    partner = [at(0, 1 - 2 * lax.rem(y, 2), 0, other), at(1, 1 - 2 * lax.rem(z, 2), 0, other)]

    def shift(flag, k):
        return MOVE[k] * flag + STAY[k] * (1 - flag)

    landing = [[at(a, shift(moved[a], k), 0, other * moved[a] + tp * (1 - moved[a])) for k in range(4)]
               for a in range(2)]

    loads = [
        pltpu.make_async_copy(wk_hbm, wk, w_sem.at[0]),
        pltpu.make_async_copy(wv_hbm, wv, w_sem.at[1]),
        pltpu.make_async_copy(rowtab_hbm.at[sp], rowtab, w_sem.at[2]),
        pltpu.make_async_copy(wq_hbm, wq, w_sem.at[3]),
        pltpu.make_async_copy(wo_hbm, wo, w_sem.at[4]),
        pltpu.make_async_copy(coltab_hbm, coltab, w_sem.at[5]),
        pltpu.make_async_copy(qgain_hbm, qgain, w_sem.at[6]),
        pltpu.make_async_copy(kgain_hbm, kgain, w_sem.at[7]),
    ]
    early = [
        pltpu.make_async_copy(tok_hbm, tok, w_sem.at[8]),
        pltpu.make_async_copy(ngain_hbm, ngain, w_sem.at[9]),
    ]
    for load in early:
        load.start()
    for load in loads:
        load.start()

    barrier = pltpu.get_barrier_semaphore()
    everyone = peers + [twin] + ring[0] + ring[1] + landing[0][1:] + landing[1][1:]
    for peer in everyone:
        pl.semaphore_signal(barrier, inc=1, device_id=peer, device_id_type=MESH)
    for a in range(2):
        @pl.when(moves[a])
        def _():
            pl.semaphore_signal(barrier, inc=1, device_id=landing[a][0], device_id_type=MESH)

    for load in early:
        load.wait()
    scaled = tok[...].astype(jnp.float32)
    inv = lax.rsqrt(jnp.mean(scaled * scaled, axis=-1, keepdims=True) + EPS)
    x[tp] = (scaled * inv * ngain[...]).astype(jnp.bfloat16)
    acc[...] = jnp.zeros_like(acc)
    lsum[...] = jnp.zeros_like(lsum)

    pl.semaphore_wait(barrier, len(everyone) + moved[0] + moved[1])

    def xcopy(i):
        slot = tp if i < N_X else lax.rem(tp + 2 * N_TP - 2 * (i - N_X + 1), N_TP)
        return pltpu.make_async_remote_copy(
            src_ref=x.at[slot], dst_ref=x.at[slot], send_sem=xs_sem.at[i], recv_sem=xr_sem.at[i],
            device_id=peers[i - 1] if 0 < i < N_X else twin, device_id_type=MESH)

    for i in (2, 1, 3, 0):
        xcopy(i).start()

    for i in (2, 5, 6, 7):
        loads[i].wait()
    for r in range(4):
        cosv[r * 64:(r + 1) * 64, :] = rowtab[r:r + 1, :] + coltab[0]
        sinv[r * 64:(r + 1) * 64, :] = rowtab[4 + r:5 + r, :] + coltab[1]

    limit = valid[0]
    lane = lax.broadcasted_iota(jnp.int32, (1, HALF), 1)

    def mask_row(slot, block, half):
        pos = block * BLOCK + half * HALF + lane
        mask[slot] = jnp.broadcast_to((pos < limit).astype(jnp.float32), (8, HALF))

    for a in range(2):
        for side in range(2):
            flag = moved[a] if side == 0 else 1 - moved[a]
            for e in range(8):
                for k in range(4):
                    place = at(a, -shift(flag, k), SOURCE[e], tp)
                    mask_row(a * 64 + side * 32 + e * 4 + k, place["sp"], a)

    loads[0].wait()
    loads[1].wait()
    for k in (1, 3, 2):
        xcopy(k).wait_recv()
        xcopy(k + N_X - 1).start()
    for i in (0, 4, 6, 5):
        xcopy(i).wait_recv()

    everything = x[...].reshape(BLOCK, x.shape[2])
    cosine = cosv[...]
    sine = sinv[...]
    in_first = (lax.broadcasted_iota(jnp.int32, (BLOCK, HEAD_DIM), 1) % 64) < 32

    def turn(projected, gain, factor):
        v = projected.astype(jnp.bfloat16).astype(jnp.float32)
        u = v * lax.rsqrt(jnp.mean(v * v, axis=-1, keepdims=True) + EPS) * gain
        moved = jnp.where(in_first, pltpu.roll(u, 96, 1), pltpu.roll(u, 32, 1))
        return (u * cosine + moved * sine) * factor

    keys = turn(jnp.dot(everything, wk[...], preferred_element_type=jnp.float32), kgain[...], 1.0)
    rows = sp * BLOCK + lax.broadcasted_iota(jnp.int32, (BLOCK, HEAD_DIM), 0)
    vals = jnp.dot(everything, wv[...], preferred_element_type=jnp.float32)
    vals = jnp.where(rows < limit, vals, 0.0).astype(jnp.bfloat16)
    for a in range(2):
        piece = slice(a * HALF, (a + 1) * HALF)
        mine[a, 0:HALF, :] = keys[piece, :].T.astype(jnp.bfloat16)
        mine[a, HALF:, :] = vals[piece, :]

    def spread(a, k):
        return pltpu.make_async_remote_copy(
            src_ref=mine.at[a], dst_ref=kv.at[a * 64 + k], send_sem=s1_sem.at[a, k], recv_sem=r1_sem.at[a, k],
            device_id=landing[a][k], device_id_type=MESH)

    def slot(a, side, e, p):
        return a * 64 + side * 32 + e * 4 + 2 * p

    def hop(a, d, p, e_from, e_to, i):
        return pltpu.make_async_remote_copy(
            src_ref=kv.at[pl.ds(slot(a, 0, e_from, p), 2)], dst_ref=kv.at[pl.ds(slot(a, 0, e_to, p), 2)],
            send_sem=s2_sem.at[a, d, i], recv_sem=r2_sem.at[a, d, i],
            device_id=ring[a][d], device_id_type=MESH)

    def share(a, e, p):
        return pltpu.make_async_remote_copy(
            src_ref=kv.at[pl.ds(slot(a, 0, e, p), 2)], dst_ref=kv.at[pl.ds(slot(a, 1, e, p), 2)],
            send_sem=st_sem.at[a, e, p], recv_sem=rt_sem.at[a, e, p],
            device_id=twin, device_id_type=MESH)

    for k in (1, 0, 2, 3):
        for a in range(2):
            if k == 0:
                @pl.when(moves[a])
                def _():
                    spread(a, 0).start()

                @pl.when(jnp.logical_not(moves[a]))
                def _():
                    kv[a * 64] = mine[a]
            else:
                spread(a, k).start()

    loads[3].wait()
    for h in range(Q_PER_KV):
        query = jnp.dot(everything, wq[:, h * HEAD_DIM:(h + 1) * HEAD_DIM], preferred_element_type=jnp.float32)
        query = turn(query, qgain[...], Q_SCALE).astype(jnp.bfloat16)
        for r in range(2):
            qs[r * 512 + h * HALF:r * 512 + (h + 1) * HALF, :] = query[r * HALF:(r + 1) * HALF, :]

    def swap_query(a):
        return pltpu.make_async_remote_copy(
            src_ref=qs, dst_ref=q.at[a], send_sem=qs_sem.at[a], recv_sem=qr_sem.at[a],
            device_id=partner[a], device_id_type=MESH)

    for a in range(2):
        @pl.when(moves[a])
        def _():
            swap_query(a).start()

        @pl.when(jnp.logical_not(moves[a]))
        def _():
            q[a] = qs[...]

    def attend(a, slots, rows):
        kt = jnp.concatenate([kv[s, 0:HALF, :] for s in slots], axis=1)
        v = jnp.concatenate([kv[s, HALF:, :] for s in slots], axis=0)
        marks = [mask[s, 0:1, :] for s in slots]
        for r in rows:
            span = pl.ds(r * 512, 512)
            s = jnp.dot(q[a, span, :], kt, preferred_element_type=jnp.float32)
            w = jnp.exp2(s)
            acc[a, span, :] += jnp.dot(w.astype(jnp.bfloat16), v, preferred_element_type=jnp.float32)
            t = w[:, 0:HALF] * marks[0]
            for i in range(1, 8):
                t = t + w[:, i * HALF:(i + 1) * HALF] * marks[i]
            lsum[a, span, :] += t

    for p in range(2):
        for a in range(2):
            if p == 0:
                @pl.when(moves[a])
                def _():
                    spread(a, 0).wait_recv()
            else:
                spread(a, 2).wait_recv()
            spread(a, 2 * p + 1).wait_recv()
            for d in range(2):
                hop(a, d, p, 0, 3 * d + 1, p).start()
            share(a, 0, p).start()

    for a in range(2):
        @pl.when(moves[a])
        def _():
            swap_query(a).wait_recv()

    def own(a, c):
        for p in range(2):
            share(a, 0, p).wait_recv()
        attend(a, [slot(a, side, 0, 0) + i for side in range(2) for i in range(4)], (0, 1))
        return c

    lax.fori_loop(0, 2, own, 0)

    def receive(i):
        e, p = i // 2 + 1, lax.rem(i, 2)
        for a in range(2):
            for d in range(2):
                hop(a, d, p, 0, 3 * d + e, i).wait_recv()

                @pl.when(i < 4)
                def _():
                    hop(a, d, p, 3 * d + e, 3 * d + e + 1, i + 2).start()

                @pl.when(i == 4 + d)
                def _():
                    hop(a, d, d, 3 * d + 3, 7, 6).start()
                share(a, 3 * d + e, p).start()

    def receive_last(d):
        for a in range(2):
            hop(a, d, d, 0, 7, 6).wait_recv()
            share(a, 7, d).start()

    def use(a, i):
        e, p = i // 2 + 1, lax.rem(i, 2)
        for d in range(2):
            share(a, 3 * d + e, p).wait_recv()
        attend(a, [slot(a, side, 3 * d + e, p) + n for side in range(2) for d in range(2) for n in range(2)], (0, 1))

    receive(jnp.int32(0))

    def stage(i, c):
        use(0, i)

        @pl.when(i < 5)
        def _():
            receive(i + 1)

        @pl.when(i == 5)
        def _():
            receive_last(0)
        use(1, i)
        return c

    lax.fori_loop(0, 6, stage, 0)
    receive_last(1)

    def give_back(a, r):
        return (
            pltpu.make_async_remote_copy(
                src_ref=o_out.at[a, r], dst_ref=o_in.at[a, r], send_sem=gs_sem.at[a, r, 0],
                recv_sem=gr_sem.at[a, r, 0], device_id=partner[a], device_id_type=MESH),
            pltpu.make_async_remote_copy(
                src_ref=l_out.at[a, r], dst_ref=l_in.at[a, r], send_sem=gs_sem.at[a, r, 1],
                recv_sem=gr_sem.at[a, r, 1], device_id=partner[a], device_id_type=MESH),
        )

    ones = jnp.ones((8, HALF), jnp.float32)

    def finish(a, r):
        span = slice(r * 512, (r + 1) * 512)
        l_out[a, r] = lax.dot_general(ones, lsum[a, span, :], (((1,), (1,)), ((), ())),
                                      precision=lax.Precision.HIGHEST, preferred_element_type=jnp.float32)

        @pl.when(moves[a])
        def _():
            o_out[a, r] = acc[a, span, :].astype(jnp.bfloat16)
            for copy in give_back(a, r):
                copy.start()

    def gather_back(r):
        span = slice(r * 512, (r + 1) * 512)
        for a in range(2):
            @pl.when(moves[a])
            def _():
                for copy in give_back(a, r):
                    copy.wait_recv()
                acc[a, span, :] = o_in[a, r].astype(jnp.float32)
                den[a, r] = l_in[a, r]

            @pl.when(jnp.logical_not(moves[a]))
            def _():
                den[a, r] = l_out[a, r]

    def final_slots(a):
        return [slot(a, side, 7, 0) + i for side in range(2) for i in range(4)]

    def project_out(r):
        totals = (den[0, r] + den[1, r]).T
        for h in range(Q_PER_KV):
            span = slice(r * 512 + h * HALF, r * 512 + (h + 1) * HALF)
            rows_of = slice(h * HALF, (h + 1) * HALF)
            att[r, :, h * HEAD_DIM:(h + 1) * HEAD_DIM] = (
                (acc[0, span, :] + acc[1, span, :]) / totals[rows_of, 0:1]).astype(jnp.bfloat16)
        mixed = jnp.dot(att[r], wo[...], preferred_element_type=jnp.float32)
        partial[4 * r:4 * r + 4] = mixed.reshape(4, ROWS, mixed.shape[1])
        for i in (2 * r, 2 * r + 1):
            to_twin[i] = partial[2 * i + 1 - core].astype(jnp.bfloat16)
            pair(i).start()

    def pair(i):
        return pltpu.make_async_remote_copy(
            src_ref=to_twin.at[i], dst_ref=from_twin.at[i], send_sem=ds_sem.at[i], recv_sem=dr_sem.at[i],
            device_id=twin, device_id_type=MESH)

    def along(i):
        return pltpu.make_async_remote_copy(
            src_ref=summed.at[i], dst_ref=arrived.at[column], send_sem=os_sem.at[i],
            recv_sem=or_sem.at[column], device_id={"sp": sp, "tp": 2 * i + core}, device_id_type=MESH)

    def arrival(source):
        return pltpu.make_async_remote_copy(
            src_ref=summed.at[0], dst_ref=arrived.at[source], send_sem=os_sem.at[0],
            recv_sem=or_sem.at[source], device_id=twin, device_id_type=MESH)

    def add_pair(i):
        pair(i).wait_recv()
        both_cores = partial[2 * i + core] + from_twin[i].astype(jnp.float32)
        partial[2 * i + core] = both_cores
        summed[i] = both_cores.astype(jnp.bfloat16)

        @pl.when(column != i)
        def _():
            along(i).start()

    for a in range(2):
        for p in range(2):
            share(a, 7, p).wait_recv()
    for r in range(2):
        for a in range(2):
            attend(a, final_slots(a), (r,))
            finish(a, r)

    loads[4].wait()
    for i in range(2 * N_X - 1):
        xcopy(i).wait_send()
    for a in range(2):
        for k in range(1, 4):
            spread(a, k).wait_send()

        @pl.when(moves[a])
        def _():
            spread(a, 0).wait_send()
            swap_query(a).wait_send()
        for d in range(2):
            for i in range(7):
                hop(a, d, 0, 0, 1, i).wait_send()
        for e in range(8):
            for p in range(2):
                share(a, e, p).wait_send()

    for r in range(2):
        gather_back(r)
        project_out(r)
        add_pair(2 * r)
        add_pair(2 * r + 1)
    total = partial[tp]
    for k in range(1, N_X):
        source = lax.rem(column + N_X - k, N_X)
        arrival(source).wait_recv()
        total = total + arrived[source].astype(jnp.float32)
    out[...] = total.astype(jnp.bfloat16)
    for a in range(2):
        @pl.when(moves[a])
        def _():
            for r in range(2):
                for copy in give_back(a, r):
                    copy.wait_send()
    for i in range(N_X):
        pair(i).wait_send()

        @pl.when(column != i)
        def _():
            along(i).wait_send()


def on_device(tokens, valid_len, norm_gain, w_query, w_key, w_value, q_gain, k_gain, w_out):
    rows, cols = rope_constants()
    width = tokens.shape[1]
    vmem = pl.BlockSpec(memory_space=pltpu.VMEM)
    anywhere = pl.BlockSpec(memory_space=pltpu.HBM)
    dma = pltpu.SemaphoreType.DMA
    call = pl.pallas_call(
        kernel,
        out_shape=jax.ShapeDtypeStruct(tokens.shape, jnp.bfloat16),
        in_specs=[anywhere, pl.BlockSpec(memory_space=pltpu.SMEM)] + [anywhere] * 9,
        out_specs=vmem,
        scratch_shapes=[
            pltpu.VMEM(tokens.shape, jnp.bfloat16),
            pltpu.VMEM((1, width), jnp.float32),
            pltpu.VMEM((1, HEAD_DIM), jnp.float32),
            pltpu.VMEM((1, HEAD_DIM), jnp.float32),
            pltpu.VMEM(cols.shape, jnp.float32),
            pltpu.VMEM((N_TP, ROWS, width), jnp.bfloat16),
            pltpu.VMEM(w_query.shape, jnp.bfloat16),
            pltpu.VMEM(w_key.shape, jnp.bfloat16),
            pltpu.VMEM(w_value.shape, jnp.bfloat16),
            pltpu.VMEM(w_out.shape, jnp.bfloat16),
            pltpu.VMEM((8, HEAD_DIM), jnp.float32),
            pltpu.VMEM((BLOCK, HEAD_DIM), jnp.float32),
            pltpu.VMEM((BLOCK, HEAD_DIM), jnp.float32),
            pltpu.VMEM((2, 2 * HALF, HEAD_DIM), jnp.bfloat16),
            pltpu.VMEM((128, 2 * HALF, HEAD_DIM), jnp.bfloat16),
            pltpu.VMEM((Q_PER_KV * BLOCK, HEAD_DIM), jnp.bfloat16),
            pltpu.VMEM((2, Q_PER_KV * BLOCK, HEAD_DIM), jnp.bfloat16),
            pltpu.VMEM((128, 8, HALF), jnp.float32),
            pltpu.VMEM((2, Q_PER_KV * BLOCK, HEAD_DIM), jnp.float32),
            pltpu.VMEM((2, Q_PER_KV * BLOCK, HEAD_DIM), jnp.float32),
            pltpu.VMEM((2, 2, 512, HEAD_DIM), jnp.bfloat16),
            pltpu.VMEM((2, 2, 512, HEAD_DIM), jnp.bfloat16),
            pltpu.VMEM((2, 2, 8, 512), jnp.float32),
            pltpu.VMEM((2, 2, 8, 512), jnp.float32),
            pltpu.VMEM((2, 2, 8, 512), jnp.float32),
            pltpu.VMEM((2, HALF, Q_PER_KV * HEAD_DIM), jnp.bfloat16),
            pltpu.VMEM((N_TP, ROWS, width), jnp.float32),
            pltpu.VMEM((N_X, ROWS, width), jnp.bfloat16),
            pltpu.VMEM((N_X, ROWS, width), jnp.bfloat16),
            pltpu.VMEM((N_X, ROWS, width), jnp.bfloat16),
            pltpu.VMEM((N_X, ROWS, width), jnp.bfloat16),
            dma((10,)), dma((7,)), dma((7,)), dma((2, 4)), dma((2, 4)), dma((2, 2, 7)), dma((2, 2, 7)),
            dma((2, 8, 2)), dma((2, 8, 2)), dma((2,)), dma((2,)), dma((2, 2, 2)), dma((2, 2, 2)),
            dma((N_X,)), dma((N_X,)), dma((N_X,)), dma((N_X,)),
        ],
        compiler_params=pltpu.CompilerParams(
            collective_id=0, has_side_effects=True, vmem_limit_bytes=67043328),
        name="fused_attention",
    )
    return call(tokens, valid_len, norm_gain.reshape(1, -1), w_query, w_key, w_value,
                q_gain.reshape(1, -1), k_gain.reshape(1, -1), w_out, jnp.asarray(rows), jnp.asarray(cols))


def solution(mesh):
    return jax.shard_map(
        on_device,
        mesh=mesh,
        in_specs=(
            P(("sp", "tp"), None),
            P(),
            P(),
            P(None, "tp"),
            P(None, "tp"),
            P(None, "tp"),
            P(),
            P(),
            P("tp", None),
        ),
        out_specs=P(("sp", "tp"), None),
        check_vma=False,
    )
```

```python
import functools
import math

import jax
import jax.numpy as jnp
import numpy as np
from jax import lax
from jax.experimental import pallas as pl
from jax.experimental.pallas import tpu as pltpu
from jax.sharding import PartitionSpec as P

HEAD_DIM = 128
Q_PER_KV = 4
GRID_W = 64
RING = 8
N_TP = 8
N_X = 4
ROWS = 32
BLOCK = 256
HALF = 128
EPS = 1e-06
MESH = pl.DeviceIdType.MESH
STAY = (0, 2, -2, 4)
MOVE = (1, -1, 3, -3)
SOURCE = (0, -1, -2, -3, 1, 2, 3, 4)
Q_SCALE = HEAD_DIM ** -0.5 * math.log2(math.e)


def rope_constants():
    freq = np.float32(10000.0) ** (-(np.arange(32, dtype=np.float32) * 2.0) / 64)
    freq = freq.astype(np.float32)
    sign = np.concatenate([-np.ones(32), np.ones(32)]).astype(np.float32)

    def table(count):
        angle = (np.arange(count, dtype=np.float32)[:, None] * freq[None, :]).astype(np.float64)
        angle = np.concatenate([angle, angle], axis=1)
        return np.cos(angle).astype(np.float32), np.sin(angle).astype(np.float32) * sign

    row_cos, row_sin = table(256)
    col_cos, col_sin = table(64)
    rows = np.zeros((64, 8, 128), np.float32)
    rows[:, 0:4, 0:64] = row_cos.reshape(64, 4, 64)
    rows[:, 4:8, 0:64] = row_sin.reshape(64, 4, 64)
    cols = np.zeros((2, 64, 128), np.float32)
    cols[0, :, 64:] = col_cos
    cols[1, :, 64:] = col_sin
    return rows, cols


def kernel(tok_hbm, valid_hbm, ngain_hbm, wq_hbm, wk_hbm, wv_hbm, qgain_hbm, kgain_hbm, wo_hbm, rowtab_hbm, coltab_hbm,
           out, tok, valid, ngain, qgain, kgain, coltab, x, wq, wk, wv, wo, rowtab, cosv, sinv, mine, kv, qs, q, mask, acc, lsum, o_out, o_in, l_out, l_in, den, att, partial, to_twin, from_twin, summed, arrived,
           w_sem, xs_sem, xr_sem, s1_sem, r1_sem, s2_sem, r2_sem,
           st_sem, rt_sem, qs_sem, qr_sem, gs_sem, gr_sem, ds_sem, dr_sem, os_sem, or_sem):
    sp = lax.axis_index("sp")
    tp = lax.axis_index("tp")
    z = sp // RING
    y = sp % RING

    def wrap(a):
        return lax.rem(a + 2 * RING, RING)

    core = lax.rem(tp, 2)
    column = tp // 2
    other = tp + 1 - 2 * core
    twin = {"sp": sp, "tp": other}
    peers = [{"sp": sp, "tp": lax.rem(tp + 2 * k, N_TP)} for k in range(1, N_X)]
    moves = (core != lax.rem(y, 2), core != lax.rem(z, 2))
    moved = [m.astype(jnp.int32) for m in moves]

    def at(part_id, first, second, where):
        dz, dy = (second, first) if part_id == 0 else (first, second)
        return {"sp": wrap(z + dz) * RING + wrap(y + dy), "tp": where}

    ring = [[at(a, 0, step, tp) for step in (1, -1)] for a in range(2)]
    partner = [at(0, 1 - 2 * lax.rem(y, 2), 0, other), at(1, 1 - 2 * lax.rem(z, 2), 0, other)]

    def shift(flag, k):
        return MOVE[k] * flag + STAY[k] * (1 - flag)

    def choose(a, if_moved, if_not):
        return if_moved * moved[a] + if_not * (1 - moved[a])

    two_on = [[at(a, step, 0, tp) for step in (2, -2)] for a in range(2)]
    landing = [[at(a, shift(moved[a], k), 0, choose(a, other, tp)) for k in range(3)]
               for a in range(2)]

    loads = [
        pltpu.make_async_copy(wk_hbm, wk, w_sem.at[0]),
        pltpu.make_async_copy(wv_hbm, wv, w_sem.at[1]),
        pltpu.make_async_copy(rowtab_hbm.at[sp], rowtab, w_sem.at[2]),
        pltpu.make_async_copy(wq_hbm, wq, w_sem.at[3]),
        pltpu.make_async_copy(wo_hbm, wo, w_sem.at[4]),
        pltpu.make_async_copy(coltab_hbm, coltab, w_sem.at[5]),
        pltpu.make_async_copy(qgain_hbm, qgain, w_sem.at[6]),
        pltpu.make_async_copy(kgain_hbm, kgain, w_sem.at[7]),
    ]
    early = [
        pltpu.make_async_copy(tok_hbm, tok, w_sem.at[8]),
        pltpu.make_async_copy(ngain_hbm, ngain, w_sem.at[9]),
        pltpu.make_async_copy(valid_hbm, valid, w_sem.at[10]),
    ]
    for load in early:
        load.start()
    for load in loads:
        load.start()

    barrier = pltpu.get_barrier_semaphore()
    everyone = peers + [twin] + ring[0] + ring[1] + two_on[0] + two_on[1]
    for peer in everyone:
        pl.semaphore_signal(barrier, inc=1, device_id=peer, device_id_type=MESH)
    for a in range(2):
        @pl.when(moves[a])
        def _():
            for k in range(2):
                pl.semaphore_signal(barrier, inc=1, device_id=landing[a][k], device_id_type=MESH)

    for load in early:
        load.wait()
    scaled = tok[...].astype(jnp.float32)
    inv = lax.rsqrt(jnp.mean(scaled * scaled, axis=-1, keepdims=True) + EPS)
    x[tp] = (scaled * inv * ngain[...]).astype(jnp.bfloat16)
    acc[...] = jnp.zeros_like(acc)
    lsum[...] = jnp.zeros_like(lsum)

    pl.semaphore_wait(barrier, len(everyone) + 2 * moved[0] + 2 * moved[1])

    def together(ref, send, recv):
        return pltpu.make_async_remote_copy(
            src_ref=ref, dst_ref=ref, send_sem=send, recv_sem=recv, device_id=twin, device_id_type=MESH)

    def xcopy(i):
        slot = tp if i < N_X else lax.rem(tp + 2 * N_TP - 2 * (i - N_X + 1), N_TP)
        return pltpu.make_async_remote_copy(
            src_ref=x.at[slot], dst_ref=x.at[slot], send_sem=xs_sem.at[0], recv_sem=xr_sem.at[i],
            device_id=peers[i - 1] if 0 < i < N_X else twin, device_id_type=MESH)

    for i in (2, 1, 3, 0):
        xcopy(i).start()

    for i in (2, 5, 6, 7):
        loads[i].wait()
    for r in range(4):
        cosv[r * 64:(r + 1) * 64, :] = rowtab[r:r + 1, :] + coltab[0]
        sinv[r * 64:(r + 1) * 64, :] = rowtab[4 + r:5 + r, :] + coltab[1]

    limit = valid[0]
    lane = lax.broadcasted_iota(jnp.int32, (1, HALF), 1)

    def mask_row(slot, block, half):
        pos = block * BLOCK + half * HALF + lane
        mask[slot] = jnp.broadcast_to((pos < limit).astype(jnp.float32), (8, HALF))

    for a in range(2):
        for side in range(2):
            flag = moved[a] if side == 0 else 1 - moved[a]
            for e in range(8):
                for k in range(4):
                    place = at(a, -shift(flag, k), SOURCE[e], tp)
                    mask_row(a * 64 + side * 32 + e * 4 + k, place["sp"], a)

    loads[0].wait()
    loads[1].wait()
    for k in (1, 3, 2):
        xcopy(k).wait_recv()
        xcopy(k + N_X - 1).start()
    for i in (0, 4, 6, 5):
        xcopy(i).wait_recv()

    everything = x[...].reshape(BLOCK, x.shape[2])
    cosine = cosv[...]
    sine = sinv[...]
    in_first = (lax.broadcasted_iota(jnp.int32, (BLOCK, HEAD_DIM), 1) % 64) < 32

    def turn(projected, gain, factor):
        v = projected.astype(jnp.bfloat16).astype(jnp.float32)
        u = v * lax.rsqrt(jnp.mean(v * v, axis=-1, keepdims=True) + EPS) * gain
        moved = jnp.where(in_first, pltpu.roll(u, 96, 1), pltpu.roll(u, 32, 1))
        return (u * cosine + moved * sine) * factor

    keys = turn(jnp.dot(everything, wk[...], preferred_element_type=jnp.float32), kgain[...], 1.0)
    rows = sp * BLOCK + lax.broadcasted_iota(jnp.int32, (BLOCK, HEAD_DIM), 0)
    vals = jnp.dot(everything, wv[...], preferred_element_type=jnp.float32)
    vals = jnp.where(rows < limit, vals, 0.0).astype(jnp.bfloat16)
    for a in range(2):
        piece = slice(a * HALF, (a + 1) * HALF)
        mine[a, 0:HALF, :] = keys[piece, :].T.astype(jnp.bfloat16)
        mine[a, HALF:, :] = vals[piece, :]

    def spread(a, k):
        return pltpu.make_async_remote_copy(
            src_ref=mine.at[a], dst_ref=kv.at[a * 64 + k], send_sem=s1_sem.at[a], recv_sem=r1_sem.at[a, k],
            device_id=landing[a][k], device_id_type=MESH)

    def pass_up(a):
        return pltpu.make_async_remote_copy(
            src_ref=kv.at[a * 64], dst_ref=kv.at[a * 64 + 2], send_sem=s1_sem.at[a], recv_sem=r1_sem.at[a, 2],
            device_id=two_on[a][0], device_id_type=MESH)

    def pass_on(a):
        odd = lax.rem((y if a == 0 else z) // 2, 2)
        upwards = odd * (1 - moved[a])
        return pltpu.make_async_remote_copy(
            src_ref=kv.at[a * 64 + choose(a, 1, 2 - odd)], dst_ref=kv.at[a * 64 + 3], send_sem=s1_sem.at[a],
            recv_sem=r1_sem.at[a, 3], device_id=at(a, 4 * upwards - 2, 0, tp), device_id_type=MESH)

    def slot(a, side, e, p):
        return a * 64 + side * 32 + e * 4 + 2 * p

    def hop(a, d, p, e_from, e_to, i):
        return pltpu.make_async_remote_copy(
            src_ref=kv.at[pl.ds(slot(a, 0, e_from, p), 2)], dst_ref=kv.at[pl.ds(slot(a, 0, e_to, p), 2)],
            send_sem=s2_sem.at[0], recv_sem=r2_sem.at[a, i + d if isinstance(i, int) and i == 6 else i],
            device_id=ring[a][d], device_id_type=MESH)

    def share(a, e, p, i):
        return pltpu.make_async_remote_copy(
            src_ref=kv.at[pl.ds(slot(a, 0, e, p), 2)], dst_ref=kv.at[pl.ds(slot(a, 1, e, p), 2)],
            send_sem=st_sem.at[0], recv_sem=rt_sem.at[a, i],
            device_id=twin, device_id_type=MESH)

    for a in range(2):
        spread(a, 1).start()

        @pl.when(moves[a])
        def _():
            spread(a, 0).start()

        @pl.when(jnp.logical_not(moves[a]))
        def _():
            spread(a, 2).start()
            kv[a * 64] = mine[a]

    loads[3].wait()
    for h in range(Q_PER_KV):
        query = jnp.dot(everything, wq[:, h * HEAD_DIM:(h + 1) * HEAD_DIM], preferred_element_type=jnp.float32)
        query = turn(query, qgain[...], Q_SCALE).astype(jnp.bfloat16)
        query = query.reshape(N_TP, 2, ROWS // 2, HEAD_DIM)
        for r in range(2):
            qs[r * 512 + h * HALF:r * 512 + (h + 1) * HALF, :] = query[:, r].reshape(HALF, HEAD_DIM)

    def swap_query(a):
        return pltpu.make_async_remote_copy(
            src_ref=qs, dst_ref=q.at[a], send_sem=qs_sem.at[a], recv_sem=qr_sem.at[a],
            device_id=partner[a], device_id_type=MESH)

    for a in range(2):
        @pl.when(moves[a])
        def _():
            swap_query(a).start()

        @pl.when(jnp.logical_not(moves[a]))
        def _():
            q[a] = qs[...]

    def attend(a, slots, rows):
        kt = jnp.concatenate([kv[s, 0:HALF, :] for s in slots], axis=1)
        v = jnp.concatenate([kv[s, HALF:, :] for s in slots], axis=0)
        marks = [mask[s, 0:1, :] for s in slots]
        for r in rows:
            span = pl.ds(r * 512, 512)
            s = jnp.dot(q[a, span, :], kt, preferred_element_type=jnp.float32)
            w = jnp.exp2(s)
            acc[a, span, :] += jnp.dot(w.astype(jnp.bfloat16), v, preferred_element_type=jnp.float32)
            t = w[:, 0:HALF] * marks[0]
            for i in range(1, len(slots)):
                t = t + w[:, i * HALF:(i + 1) * HALF] * marks[i]
            lsum[a, span, :] += t

    def hand_on(a, p):
        for d in range(2):
            hop(a, d, p, 0, 3 * d + 1, p).start()
        share(a, 0, p, p).start()

    for a in range(2):
        @pl.when(moves[a])
        def _():
            spread(a, 0).wait_recv()
            pass_up(a).start()
        spread(a, 1).wait_recv()

        @pl.when(jnp.logical_not(moves[a]))
        def _():
            spread(a, 2).wait_recv()
        pass_on(a).start()
    for a in range(2):
        hand_on(a, 0)

    for a in range(2):
        @pl.when(moves[a])
        def _():
            swap_query(a).wait_recv()

    def own(a, p):
        share(a, 0, p, p).wait_recv()
        attend(a, [slot(a, side, 0, p) + i for side in range(2) for i in range(2)], (0, 1))

    for a in range(2):
        own(a, 0)
    for a in range(2):
        @pl.when(moves[a])
        def _():
            pass_up(a).wait_recv()
        pass_on(a).wait_recv()
        hand_on(a, 1)

    def receive(i):
        e, p = i // 2 + 1, lax.rem(i, 2)
        for a in range(2):
            together(kv.at[pl.ds(a * 64, 4)], s2_sem.at[0], r2_sem.at[a, i]).wait_recv()
            for d in range(2):
                @pl.when(i < 4)
                def _():
                    hop(a, d, p, 3 * d + e, 3 * d + e + 1, i + 2).start()

                @pl.when(i == 4 + d)
                def _():
                    hop(a, d, d, 3 * d + 3, 7, 6).start()
                share(a, 3 * d + e, p, i + 2).start()

    def receive_last(d):
        for a in range(2):
            hop(a, d, d, 0, 7, 6).wait_recv()
            share(a, 7, d, 8 + d).start()

    def use(a, i):
        e, p = i // 2 + 1, lax.rem(i, 2)
        together(kv.at[pl.ds(a * 64, 4)], st_sem.at[0], rt_sem.at[a, i + 2]).wait_recv()
        attend(a, [slot(a, side, 3 * d + e, p) + n for side in range(2) for d in range(2) for n in range(2)], (0, 1))

    own(0, 1)
    receive(jnp.int32(0))
    own(1, 1)

    def stage(i, c):
        use(0, i)

        @pl.when(i < 5)
        def _():
            receive(i + 1)

        @pl.when(i == 5)
        def _():
            receive_last(0)
        use(1, i)
        return c

    lax.fori_loop(0, 6, stage, 0)

    def final_slots(a, p):
        share(a, 7, p, 8 + p).wait_recv()
        return [slot(a, side, 7, p) + i for side in range(2) for i in range(2)]

    attend(0, final_slots(0, 0), (0, 1))
    receive_last(1)
    attend(1, final_slots(1, 0), (0, 1))

    def give_back(a, r):
        return (
            pltpu.make_async_remote_copy(
                src_ref=o_out.at[a, r], dst_ref=o_in.at[a, r], send_sem=gs_sem.at[a, 0],
                recv_sem=gr_sem.at[a, r, 0], device_id=partner[a], device_id_type=MESH),
            pltpu.make_async_remote_copy(
                src_ref=l_out.at[a, r], dst_ref=l_in.at[a, r], send_sem=gs_sem.at[a, 1],
                recv_sem=gr_sem.at[a, r, 1], device_id=partner[a], device_id_type=MESH),
        )

    ones = jnp.ones((8, HALF), jnp.bfloat16)

    def finish(a, r):
        span = slice(r * 512, (r + 1) * 512)
        sums = lsum[a, span, :]
        high = sums.astype(jnp.bfloat16)
        low = (sums - high.astype(jnp.float32)).astype(jnp.bfloat16)
        across = (((1,), (1,)), ((), ()))
        l_out[a, r] = (lax.dot_general(ones, high, across, preferred_element_type=jnp.float32)
                       + lax.dot_general(ones, low, across, preferred_element_type=jnp.float32))

        @pl.when(moves[a])
        def _():
            o_out[a, r] = acc[a, span, :].astype(jnp.bfloat16)
            for copy in give_back(a, r):
                copy.start()

    def gather_back(r):
        span = slice(r * 512, (r + 1) * 512)
        for a in range(2):
            @pl.when(moves[a])
            def _():
                for copy in give_back(a, r):
                    copy.wait_recv()
                acc[a, span, :] = o_in[a, r].astype(jnp.float32)
                den[a, r] = l_in[a, r]

            @pl.when(jnp.logical_not(moves[a]))
            def _():
                den[a, r] = l_out[a, r]

    def project_out(r):
        totals = (den[0, r] + den[1, r]).T
        for h in range(Q_PER_KV):
            span = slice(r * 512 + h * HALF, r * 512 + (h + 1) * HALF)
            rows_of = slice(h * HALF, (h + 1) * HALF)
            att[r, :, h * HEAD_DIM:(h + 1) * HEAD_DIM] = (
                (acc[0, span, :] + acc[1, span, :]) / totals[rows_of, 0:1]).astype(jnp.bfloat16)
        mixed = jnp.dot(att[r], wo[...], preferred_element_type=jnp.float32)
        part_rows = slice(r * ROWS // 2, (r + 1) * ROWS // 2)
        partial[:, part_rows, :] = mixed.reshape(N_TP, ROWS // 2, mixed.shape[1])
        for i in range(N_X):
            to_twin[r, i] = partial[2 * i + 1 - core, part_rows, :].astype(jnp.bfloat16)
        pair(r).start()

    def pair(r):
        return pltpu.make_async_remote_copy(
            src_ref=to_twin.at[r], dst_ref=from_twin.at[r], send_sem=ds_sem.at[r], recv_sem=dr_sem.at[r],
            device_id=twin, device_id_type=MESH)

    def along(r, i):
        return pltpu.make_async_remote_copy(
            src_ref=summed.at[r, i], dst_ref=arrived.at[r, column], send_sem=os_sem.at[r],
            recv_sem=or_sem.at[r], device_id={"sp": sp, "tp": 2 * i + core}, device_id_type=MESH)

    def add_pair(r):
        pair(r).wait_recv()
        part_rows = slice(r * ROWS // 2, (r + 1) * ROWS // 2)
        for i in range(N_X):
            both_cores = partial[2 * i + core, part_rows, :] + from_twin[r, i].astype(jnp.float32)
            partial[2 * i + core, part_rows, :] = both_cores
            summed[r, i] = both_cores.astype(jnp.bfloat16)

            @pl.when(column != i)
            def _():
                along(r, i).start()

    slots = [final_slots(a, 1) for a in range(2)]
    for r in range(2):
        for a in range(2):
            attend(a, slots[a], (r,))
            finish(a, r)

    loads[4].wait()
    together(x.at[pl.ds(0, 2 * N_X - 1)], xs_sem.at[0], xr_sem.at[0]).wait_send()
    for a in range(2):
        @pl.when(moves[a])
        def _():
            together(kv.at[pl.ds(0, 4)], s1_sem.at[a], r1_sem.at[a, 0]).wait_send()
            swap_query(a).wait_send()

        @pl.when(jnp.logical_not(moves[a]))
        def _():
            together(kv.at[pl.ds(0, 3)], s1_sem.at[a], r1_sem.at[a, 0]).wait_send()
    together(kv.at[pl.ds(0, 56)], s2_sem.at[0], r2_sem.at[0, 0]).wait_send()
    together(kv.at[pl.ds(0, 64)], st_sem.at[0], rt_sem.at[0, 0]).wait_send()

    gather_back(0)
    project_out(0)
    gather_back(1)
    add_pair(0)
    project_out(1)
    add_pair(1)
    for r in range(2):
        part_rows = slice(r * ROWS // 2, (r + 1) * ROWS // 2)
        total = partial[tp, part_rows, :]
        together(arrived.at[r, pl.ds(0, N_X - 1)], os_sem.at[r], or_sem.at[r]).wait_recv()
        for k in range(1, N_X):
            total = total + arrived[r, lax.rem(column + N_X - k, N_X)].astype(jnp.float32)
        out[part_rows, :] = total.astype(jnp.bfloat16)
    for a in range(2):
        @pl.when(moves[a])
        def _():
            together(o_out.at[a], gs_sem.at[a, 0], gr_sem.at[a, 0, 0]).wait_send()
            together(l_out.at[a], gs_sem.at[a, 1], gr_sem.at[a, 0, 1]).wait_send()
    for r in range(2):
        pair(r).wait_send()
        together(summed.at[r, pl.ds(0, N_X - 1)], os_sem.at[r], or_sem.at[r]).wait_send()


def on_device(tokens, valid_len, norm_gain, w_query, w_key, w_value, q_gain, k_gain, w_out):
    rows, cols = rope_constants()
    width = tokens.shape[1]
    vmem = pl.BlockSpec(memory_space=pltpu.VMEM)
    anywhere = pl.BlockSpec(memory_space=pltpu.HBM)
    dma = pltpu.SemaphoreType.DMA
    call = pl.pallas_call(
        kernel,
        out_shape=jax.ShapeDtypeStruct(tokens.shape, jnp.bfloat16),
        in_specs=[anywhere] * 11,
        out_specs=vmem,
        scratch_shapes=[
            pltpu.VMEM(tokens.shape, jnp.bfloat16),
            pltpu.SMEM((1,), jnp.int32),
            pltpu.VMEM((1, width), jnp.float32),
            pltpu.VMEM((1, HEAD_DIM), jnp.float32),
            pltpu.VMEM((1, HEAD_DIM), jnp.float32),
            pltpu.VMEM(cols.shape, jnp.float32),
            pltpu.VMEM((N_TP, ROWS, width), jnp.bfloat16),
            pltpu.VMEM(w_query.shape, jnp.bfloat16),
            pltpu.VMEM(w_key.shape, jnp.bfloat16),
            pltpu.VMEM(w_value.shape, jnp.bfloat16),
            pltpu.VMEM(w_out.shape, jnp.bfloat16),
            pltpu.VMEM((8, HEAD_DIM), jnp.float32),
            pltpu.VMEM((BLOCK, HEAD_DIM), jnp.float32),
            pltpu.VMEM((BLOCK, HEAD_DIM), jnp.float32),
            pltpu.VMEM((2, 2 * HALF, HEAD_DIM), jnp.bfloat16),
            pltpu.VMEM((128, 2 * HALF, HEAD_DIM), jnp.bfloat16),
            pltpu.VMEM((Q_PER_KV * BLOCK, HEAD_DIM), jnp.bfloat16),
            pltpu.VMEM((2, Q_PER_KV * BLOCK, HEAD_DIM), jnp.bfloat16),
            pltpu.VMEM((128, 8, HALF), jnp.float32),
            pltpu.VMEM((2, Q_PER_KV * BLOCK, HEAD_DIM), jnp.float32),
            pltpu.VMEM((2, Q_PER_KV * BLOCK, HEAD_DIM), jnp.float32),
            pltpu.VMEM((2, 2, 512, HEAD_DIM), jnp.bfloat16),
            pltpu.VMEM((2, 2, 512, HEAD_DIM), jnp.bfloat16),
            pltpu.VMEM((2, 2, 8, 512), jnp.float32),
            pltpu.VMEM((2, 2, 8, 512), jnp.float32),
            pltpu.VMEM((2, 2, 8, 512), jnp.float32),
            pltpu.VMEM((2, HALF, Q_PER_KV * HEAD_DIM), jnp.bfloat16),
            pltpu.VMEM((N_TP, ROWS, width), jnp.float32),
            pltpu.VMEM((2, N_X, ROWS // 2, width), jnp.bfloat16),
            pltpu.VMEM((2, N_X, ROWS // 2, width), jnp.bfloat16),
            pltpu.VMEM((2, N_X, ROWS // 2, width), jnp.bfloat16),
            pltpu.VMEM((2, N_X, ROWS // 2, width), jnp.bfloat16),
            dma((11,)), dma((1,)), dma((7,)), dma((2,)), dma((2, 4)), dma((1,)), dma((2, 8)),
            dma((1,)), dma((2, 10)), dma((2,)), dma((2,)), dma((2, 2)), dma((2, 2, 2)),
            dma((2,)), dma((2,)), dma((2,)), dma((2,)),
        ],
        compiler_params=pltpu.CompilerParams(
            collective_id=0, has_side_effects=True, vmem_limit_bytes=67043328),
        name="fused_attention",
    )
    return call(tokens, valid_len, norm_gain.reshape(1, -1), w_query, w_key, w_value,
                q_gain.reshape(1, -1), k_gain.reshape(1, -1), w_out, jnp.asarray(rows), jnp.asarray(cols))


def solution(mesh):
    return jax.shard_map(
        on_device,
        mesh=mesh,
        in_specs=(
            P(("sp", "tp"), None),
            P(),
            P(),
            P(None, "tp"),
            P(None, "tp"),
            P(None, "tp"),
            P(),
            P(),
            P("tp", None),
        ),
        out_specs=P(("sp", "tp"), None),
        check_vma=False,
    )
```

```python
import functools
import math

import jax
import jax.numpy as jnp
import numpy as np
from jax import lax
from jax.experimental import pallas as pl
from jax.experimental.pallas import tpu as pltpu
from jax.sharding import PartitionSpec as P

HEAD_DIM = 128
Q_PER_KV = 4
GRID_W = 64
RING = 8
N_TP = 8
N_X = 4
ROWS = 32
BLOCK = 256
HALF = 128
EPS = 1e-06
MESH = pl.DeviceIdType.MESH
STAY = (0, 2, -2, 4)
MOVE = (1, -1, 3, -3)
SOURCE = (0, -1, -2, -3, 1, 2, 3, 4)
Q_SCALE = HEAD_DIM ** -0.5 * math.log2(math.e)


def rope_constants():
    freq = np.float32(10000.0) ** (-(np.arange(32, dtype=np.float32) * 2.0) / 64)
    freq = freq.astype(np.float32)
    sign = np.concatenate([-np.ones(32), np.ones(32)]).astype(np.float32)

    def table(count):
        angle = (np.arange(count, dtype=np.float32)[:, None] * freq[None, :]).astype(np.float64)
        angle = np.concatenate([angle, angle], axis=1)
        return np.cos(angle).astype(np.float32), np.sin(angle).astype(np.float32) * sign

    row_cos, row_sin = table(256)
    col_cos, col_sin = table(64)
    rows = np.zeros((64, 8, 128), np.float32)
    rows[:, 0:4, 0:64] = row_cos.reshape(64, 4, 64)
    rows[:, 4:8, 0:64] = row_sin.reshape(64, 4, 64)
    cols = np.zeros((2, 64, 128), np.float32)
    cols[0, :, 64:] = col_cos
    cols[1, :, 64:] = col_sin
    return rows, cols


def kernel(tok_hbm, valid_hbm, ngain_hbm, wq_hbm, wk_hbm, wv_hbm, qgain_hbm, kgain_hbm, wo_hbm, rowtab_hbm, coltab_hbm,
           out, tok, valid, ngain, qgain, kgain, coltab, x, wq, wk, wv, wo, rowtab, cosv, sinv, mine, kv, qs, q, mask, acc, lsum, o_out, o_in, l_out, l_in, den, att, partial, to_twin, from_twin, summed, arrived,
           w_sem, xs_sem, xr_sem, s1_sem, r1_sem, s2_sem, r2_sem,
           st_sem, rt_sem, qs_sem, qr_sem, gs_sem, gr_sem, ds_sem, dr_sem, os_sem, or_sem):
    sp = lax.axis_index("sp")
    tp = lax.axis_index("tp")
    z = sp // RING
    y = sp % RING

    def wrap(a):
        return lax.rem(a + 2 * RING, RING)

    core = lax.rem(tp, 2)
    column = tp // 2
    other = tp + 1 - 2 * core
    twin = {"sp": sp, "tp": other}
    peers = [{"sp": sp, "tp": lax.rem(tp + 2 * k, N_TP)} for k in range(1, N_X)]
    moves = (core != lax.rem(y, 2), core != lax.rem(z, 2))
    moved = [m.astype(jnp.int32) for m in moves]

    def at(part_id, first, second, where):
        dz, dy = (second, first) if part_id == 0 else (first, second)
        return {"sp": wrap(z + dz) * RING + wrap(y + dy), "tp": where}

    ring = [[at(a, 0, step, tp) for step in (1, -1)] for a in range(2)]
    partner = [at(0, 1 - 2 * lax.rem(y, 2), 0, other), at(1, 1 - 2 * lax.rem(z, 2), 0, other)]

    def shift(flag, k):
        return MOVE[k] * flag + STAY[k] * (1 - flag)

    def choose(a, if_moved, if_not):
        return if_moved * moved[a] + if_not * (1 - moved[a])

    two_on = [[at(a, step, 0, tp) for step in (2, -2)] for a in range(2)]
    landing = [[at(a, shift(moved[a], k), 0, choose(a, other, tp)) for k in range(3)]
               for a in range(2)]

    loads = [
        pltpu.make_async_copy(wk_hbm, wk, w_sem.at[0]),
        pltpu.make_async_copy(wv_hbm, wv, w_sem.at[1]),
        pltpu.make_async_copy(rowtab_hbm.at[sp], rowtab, w_sem.at[2]),
        pltpu.make_async_copy(wq_hbm, wq, w_sem.at[3]),
        pltpu.make_async_copy(wo_hbm, wo, w_sem.at[4]),
        pltpu.make_async_copy(coltab_hbm, coltab, w_sem.at[5]),
        pltpu.make_async_copy(qgain_hbm, qgain, w_sem.at[6]),
        pltpu.make_async_copy(kgain_hbm, kgain, w_sem.at[7]),
    ]
    early = [
        pltpu.make_async_copy(tok_hbm, tok, w_sem.at[8]),
        pltpu.make_async_copy(ngain_hbm, ngain, w_sem.at[9]),
        pltpu.make_async_copy(valid_hbm, valid, w_sem.at[10]),
    ]
    for load in early:
        load.start()
    for load in loads:
        load.start()

    barrier = pltpu.get_barrier_semaphore()
    everyone = peers + [twin] + ring[0] + ring[1] + two_on[0] + two_on[1]
    for peer in everyone:
        pl.semaphore_signal(barrier, inc=1, device_id=peer, device_id_type=MESH)
    for a in range(2):
        @pl.when(moves[a])
        def _():
            for k in range(2):
                pl.semaphore_signal(barrier, inc=1, device_id=landing[a][k], device_id_type=MESH)

    for load in early:
        load.wait()
    scaled = tok[...].astype(jnp.float32)
    inv = lax.rsqrt(jnp.mean(scaled * scaled, axis=-1, keepdims=True) + EPS)
    x[tp] = (scaled * inv * ngain[...]).astype(jnp.bfloat16)
    acc[...] = jnp.zeros_like(acc)
    lsum[...] = jnp.zeros_like(lsum)

    pl.semaphore_wait(barrier, len(everyone) + 2 * moved[0] + 2 * moved[1])

    def together(ref, send, recv):
        return pltpu.make_async_remote_copy(
            src_ref=ref, dst_ref=ref, send_sem=send, recv_sem=recv, device_id=twin, device_id_type=MESH)

    def xcopy(i):
        slot = tp if i < N_X else lax.rem(tp + 2 * N_TP - 2 * (i - N_X + 1), N_TP)
        return pltpu.make_async_remote_copy(
            src_ref=x.at[slot], dst_ref=x.at[slot], send_sem=xs_sem.at[0], recv_sem=xr_sem.at[i],
            device_id=peers[i - 1] if 0 < i < N_X else twin, device_id_type=MESH)

    for i in (2, 1, 3, 0):
        xcopy(i).start()

    for i in (2, 5, 6, 7):
        loads[i].wait()
    for r in range(4):
        cosv[r * 64:(r + 1) * 64, :] = rowtab[r:r + 1, :] + coltab[0]
        sinv[r * 64:(r + 1) * 64, :] = rowtab[4 + r:5 + r, :] + coltab[1]

    limit = valid[0]
    lane = lax.broadcasted_iota(jnp.int32, (1, HALF), 1)

    def mask_row(slot, block, half):
        pos = block * BLOCK + half * HALF + lane
        mask[slot] = jnp.broadcast_to((pos < limit).astype(jnp.float32), (8, HALF))

    for a in range(2):
        for side in range(2):
            flag = moved[a] if side == 0 else 1 - moved[a]
            for e in range(8):
                for k in range(4):
                    place = at(a, -shift(flag, k), SOURCE[e], tp)
                    mask_row(a * 64 + side * 32 + e * 4 + k, place["sp"], a)

    loads[0].wait()
    loads[1].wait()
    for k in (1, 3, 2):
        xcopy(k).wait_recv()
        xcopy(k + N_X - 1).start()
    for i in (0, 4, 6, 5):
        xcopy(i).wait_recv()

    everything = x[...].reshape(BLOCK, x.shape[2])
    cosine = cosv[...]
    sine = sinv[...]
    in_first = (lax.broadcasted_iota(jnp.int32, (BLOCK, HEAD_DIM), 1) % 64) < 32

    def turn(projected, gain, factor):
        v = projected.astype(jnp.bfloat16).astype(jnp.float32)
        u = v * lax.rsqrt(jnp.mean(v * v, axis=-1, keepdims=True) + EPS) * gain
        moved = jnp.where(in_first, pltpu.roll(u, 96, 1), pltpu.roll(u, 32, 1))
        return (u * cosine + moved * sine) * factor

    keys = turn(jnp.dot(everything, wk[...], preferred_element_type=jnp.float32), kgain[...], 1.0)
    rows = sp * BLOCK + lax.broadcasted_iota(jnp.int32, (BLOCK, HEAD_DIM), 0)
    vals = jnp.dot(everything, wv[...], preferred_element_type=jnp.float32)
    vals = jnp.where(rows < limit, vals, 0.0).astype(jnp.bfloat16)
    for a in range(2):
        piece = slice(a * HALF, (a + 1) * HALF)
        mine[a, 0:HALF, :] = keys[piece, :].T.astype(jnp.bfloat16)
        mine[a, HALF:, :] = vals[piece, :]

    def spread(a, k):
        return pltpu.make_async_remote_copy(
            src_ref=mine.at[a], dst_ref=kv.at[a * 64 + k], send_sem=s1_sem.at[a], recv_sem=r1_sem.at[a, k],
            device_id=landing[a][k], device_id_type=MESH)

    def pass_up(a):
        return pltpu.make_async_remote_copy(
            src_ref=kv.at[a * 64], dst_ref=kv.at[a * 64 + 2], send_sem=s1_sem.at[a], recv_sem=r1_sem.at[a, 2],
            device_id=two_on[a][0], device_id_type=MESH)

    def pass_on(a):
        odd = lax.rem((y if a == 0 else z) // 2, 2)
        upwards = odd * (1 - moved[a])
        return pltpu.make_async_remote_copy(
            src_ref=kv.at[a * 64 + choose(a, 1, 2 - odd)], dst_ref=kv.at[a * 64 + 3], send_sem=s1_sem.at[a],
            recv_sem=r1_sem.at[a, 3], device_id=at(a, 4 * upwards - 2, 0, tp), device_id_type=MESH)

    def slot(a, side, e, p):
        return a * 64 + side * 32 + e * 4 + 2 * p

    def hop(a, d, p, e_from, e_to, i):
        return pltpu.make_async_remote_copy(
            src_ref=kv.at[pl.ds(slot(a, 0, e_from, p), 2)], dst_ref=kv.at[pl.ds(slot(a, 0, e_to, p), 2)],
            send_sem=s2_sem.at[0], recv_sem=r2_sem.at[a, i + d if isinstance(i, int) and i == 6 else i],
            device_id=ring[a][d], device_id_type=MESH)

    def share(a, e, p, i):
        return pltpu.make_async_remote_copy(
            src_ref=kv.at[pl.ds(slot(a, 0, e, p), 2)], dst_ref=kv.at[pl.ds(slot(a, 1, e, p), 2)],
            send_sem=st_sem.at[0], recv_sem=rt_sem.at[a, i],
            device_id=twin, device_id_type=MESH)

    for a in range(2):
        spread(a, 1).start()

        @pl.when(moves[a])
        def _():
            spread(a, 0).start()

        @pl.when(jnp.logical_not(moves[a]))
        def _():
            spread(a, 2).start()
            kv[a * 64] = mine[a]

    loads[3].wait()
    for h in range(Q_PER_KV):
        query = jnp.dot(everything, wq[:, h * HEAD_DIM:(h + 1) * HEAD_DIM], preferred_element_type=jnp.float32)
        query = turn(query, qgain[...], Q_SCALE).astype(jnp.bfloat16)
        query = query.reshape(N_TP, 2, ROWS // 2, HEAD_DIM)
        for r in range(2):
            qs[r * 512 + h * HALF:r * 512 + (h + 1) * HALF, :] = query[:, r].reshape(HALF, HEAD_DIM)

    def swap_query(a):
        return pltpu.make_async_remote_copy(
            src_ref=qs, dst_ref=q.at[a], send_sem=qs_sem.at[a], recv_sem=qr_sem.at[a],
            device_id=partner[a], device_id_type=MESH)

    for a in range(2):
        @pl.when(moves[a])
        def _():
            swap_query(a).start()

        @pl.when(jnp.logical_not(moves[a]))
        def _():
            q[a] = qs[...]

    def attend(a, slots, rows):
        kt = jnp.concatenate([kv[s, 0:HALF, :] for s in slots], axis=1)
        v = jnp.concatenate([kv[s, HALF:, :] for s in slots], axis=0)
        marks = [mask[s, 0:1, :] for s in slots]
        for r in rows:
            span = pl.ds(r * 512, 512)
            s = jnp.dot(q[a, span, :], kt, preferred_element_type=jnp.float32)
            w = jnp.exp2(s)
            acc[a, span, :] += jnp.dot(w.astype(jnp.bfloat16), v, preferred_element_type=jnp.float32)
            t = w[:, 0:HALF] * marks[0]
            for i in range(1, len(slots)):
                t = t + w[:, i * HALF:(i + 1) * HALF] * marks[i]
            lsum[a, span, :] += t

    def hand_on(a, p):
        for d in range(2):
            hop(a, d, p, 0, 3 * d + 1, p).start()
        share(a, 0, p, p).start()

    for a in range(2):
        @pl.when(moves[a])
        def _():
            spread(a, 0).wait_recv()
            pass_up(a).start()
        spread(a, 1).wait_recv()

        @pl.when(jnp.logical_not(moves[a]))
        def _():
            spread(a, 2).wait_recv()
        pass_on(a).start()
    for a in range(2):
        hand_on(a, 0)

    for a in range(2):
        @pl.when(moves[a])
        def _():
            swap_query(a).wait_recv()

    def own(a, p):
        share(a, 0, p, p).wait_recv()
        attend(a, [slot(a, side, 0, p) + i for side in range(2) for i in range(2)], (0, 1))

    for a in range(2):
        own(a, 0)
    for a in range(2):
        @pl.when(moves[a])
        def _():
            pass_up(a).wait_recv()
        pass_on(a).wait_recv()
        hand_on(a, 1)

    def receive(i):
        e, p = i // 2 + 1, lax.rem(i, 2)
        for a in range(2):
            together(kv.at[pl.ds(a * 64, 4)], s2_sem.at[0], r2_sem.at[a, i]).wait_recv()
            for d in range(2):
                @pl.when(i < 4)
                def _():
                    hop(a, d, p, 3 * d + e, 3 * d + e + 1, i + 2).start()

                @pl.when(i == 4 + d)
                def _():
                    hop(a, d, d, 3 * d + 3, 7, 6).start()
                share(a, 3 * d + e, p, i + 2).start()

    def receive_last(d):
        for a in range(2):
            hop(a, d, d, 0, 7, 6).wait_recv()
            share(a, 7, d, 8 + d).start()

    def use(a, i):
        e, p = i // 2 + 1, lax.rem(i, 2)
        together(kv.at[pl.ds(a * 64, 4)], st_sem.at[0], rt_sem.at[a, i + 2]).wait_recv()
        attend(a, [slot(a, side, 3 * d + e, p) + n for side in range(2) for d in range(2) for n in range(2)], (0, 1))

    own(0, 1)
    receive(jnp.int32(0))
    own(1, 1)

    def stage(i, c):
        use(0, i)

        @pl.when(i < 5)
        def _():
            receive(i + 1)

        @pl.when(i == 5)
        def _():
            receive_last(0)
        use(1, i)
        return c

    lax.fori_loop(0, 6, stage, 0)

    def final_slots(a, p):
        share(a, 7, p, 8 + p).wait_recv()
        return [slot(a, side, 7, p) + i for side in range(2) for i in range(2)]

    attend(0, final_slots(0, 0), (0, 1))
    receive_last(1)
    attend(1, final_slots(1, 0), (0, 1))

    def give_back(a, r):
        return (
            pltpu.make_async_remote_copy(
                src_ref=o_out.at[a, r], dst_ref=o_in.at[a, r], send_sem=gs_sem.at[a, 0],
                recv_sem=gr_sem.at[a, r, 0], device_id=partner[a], device_id_type=MESH),
            pltpu.make_async_remote_copy(
                src_ref=l_out.at[a, r], dst_ref=l_in.at[a, r], send_sem=gs_sem.at[a, 1],
                recv_sem=gr_sem.at[a, r, 1], device_id=partner[a], device_id_type=MESH),
        )

    ones = jnp.ones((8, HALF), jnp.bfloat16)

    def finish(a, r):
        span = slice(r * 512, (r + 1) * 512)
        sums = lsum[a, span, :]
        high = sums.astype(jnp.bfloat16)
        low = (sums - high.astype(jnp.float32)).astype(jnp.bfloat16)
        across = (((1,), (1,)), ((), ()))
        l_out[a, r] = (lax.dot_general(ones, high, across, preferred_element_type=jnp.float32)
                       + lax.dot_general(ones, low, across, preferred_element_type=jnp.float32))

        @pl.when(moves[a])
        def _():
            o_out[a, r] = acc[a, span, :].astype(jnp.bfloat16)
            for copy in give_back(a, r):
                copy.start()

    def gather_back(r):
        span = slice(r * 512, (r + 1) * 512)
        for a in range(2):
            @pl.when(moves[a])
            def _():
                for copy in give_back(a, r):
                    copy.wait_recv()
                acc[a, span, :] = o_in[a, r].astype(jnp.float32)
                den[a, r] = l_in[a, r]

            @pl.when(jnp.logical_not(moves[a]))
            def _():
                den[a, r] = l_out[a, r]

    def project_out(r):
        totals = (den[0, r] + den[1, r]).T
        for h in range(Q_PER_KV):
            span = slice(r * 512 + h * HALF, r * 512 + (h + 1) * HALF)
            rows_of = slice(h * HALF, (h + 1) * HALF)
            att[r, :, h * HEAD_DIM:(h + 1) * HEAD_DIM] = (
                (acc[0, span, :] + acc[1, span, :]) / totals[rows_of, 0:1]).astype(jnp.bfloat16)
        mixed = jnp.dot(att[r], wo[...], preferred_element_type=jnp.float32)
        part_rows = slice(r * ROWS // 2, (r + 1) * ROWS // 2)
        partial[:, part_rows, :] = mixed.reshape(N_TP, ROWS // 2, mixed.shape[1])
        for i in range(N_X):
            to_twin[r, i] = partial[2 * i + 1 - core, part_rows, :].astype(jnp.bfloat16)
        pair(r).start()

    def pair(r):
        return pltpu.make_async_remote_copy(
            src_ref=to_twin.at[r], dst_ref=from_twin.at[r], send_sem=ds_sem.at[r], recv_sem=dr_sem.at[r],
            device_id=twin, device_id_type=MESH)

    def along(r, i):
        return pltpu.make_async_remote_copy(
            src_ref=summed.at[r, i], dst_ref=arrived.at[r, column], send_sem=os_sem.at[r],
            recv_sem=or_sem.at[r], device_id={"sp": sp, "tp": 2 * i + core}, device_id_type=MESH)

    def add_pair(r):
        pair(r).wait_recv()
        part_rows = slice(r * ROWS // 2, (r + 1) * ROWS // 2)
        for i in range(N_X):
            both_cores = partial[2 * i + core, part_rows, :] + from_twin[r, i].astype(jnp.float32)
            partial[2 * i + core, part_rows, :] = both_cores
            summed[r, i] = both_cores.astype(jnp.bfloat16)

            @pl.when(column != i)
            def _():
                along(r, i).start()

    slots = [final_slots(a, 1) for a in range(2)]
    for r in range(2):
        for a in range(2):
            attend(a, slots[a], (r,))
            finish(a, r)

    loads[4].wait()
    together(x.at[pl.ds(0, 2 * N_X - 1)], xs_sem.at[0], xr_sem.at[0]).wait_send()
    for a in range(2):
        @pl.when(moves[a])
        def _():
            together(kv.at[pl.ds(0, 4)], s1_sem.at[a], r1_sem.at[a, 0]).wait_send()
            swap_query(a).wait_send()

        @pl.when(jnp.logical_not(moves[a]))
        def _():
            together(kv.at[pl.ds(0, 3)], s1_sem.at[a], r1_sem.at[a, 0]).wait_send()
    together(kv.at[pl.ds(0, 56)], s2_sem.at[0], r2_sem.at[0, 0]).wait_send()
    together(kv.at[pl.ds(0, 64)], st_sem.at[0], rt_sem.at[0, 0]).wait_send()

    gather_back(0)
    project_out(0)
    gather_back(1)
    add_pair(0)
    project_out(1)
    add_pair(1)
    for r in range(2):
        part_rows = slice(r * ROWS // 2, (r + 1) * ROWS // 2)
        total = partial[tp, part_rows, :]
        together(arrived.at[r, pl.ds(0, N_X - 1)], os_sem.at[r], or_sem.at[r]).wait_recv()
        for k in range(1, N_X):
            total = total + arrived[r, lax.rem(column + N_X - k, N_X)].astype(jnp.float32)
        out[part_rows, :] = total.astype(jnp.bfloat16)
    for a in range(2):
        @pl.when(moves[a])
        def _():
            together(o_out.at[a], gs_sem.at[a, 0], gr_sem.at[a, 0, 0]).wait_send()
            together(l_out.at[a], gs_sem.at[a, 1], gr_sem.at[a, 0, 1]).wait_send()
    for r in range(2):
        pair(r).wait_send()
        together(summed.at[r, pl.ds(0, N_X - 1)], os_sem.at[r], or_sem.at[r]).wait_send()


def on_device(tokens, valid_len, norm_gain, w_query, w_key, w_value, q_gain, k_gain, w_out):
    rows, cols = rope_constants()
    width = tokens.shape[1]
    vmem = pl.BlockSpec(memory_space=pltpu.VMEM)
    anywhere = pl.BlockSpec(memory_space=pltpu.HBM)
    dma = pltpu.SemaphoreType.DMA
    call = pl.pallas_call(
        kernel,
        out_shape=jax.ShapeDtypeStruct(tokens.shape, jnp.bfloat16),
        in_specs=[anywhere] * 11,
        out_specs=vmem,
        scratch_shapes=[
            pltpu.VMEM(tokens.shape, jnp.bfloat16),
            pltpu.SMEM((1,), jnp.int32),
            pltpu.VMEM((1, width), jnp.float32),
            pltpu.VMEM((1, HEAD_DIM), jnp.float32),
            pltpu.VMEM((1, HEAD_DIM), jnp.float32),
            pltpu.VMEM(cols.shape, jnp.float32),
            pltpu.VMEM((N_TP, ROWS, width), jnp.bfloat16),
            pltpu.VMEM(w_query.shape, jnp.bfloat16),
            pltpu.VMEM(w_key.shape, jnp.bfloat16),
            pltpu.VMEM(w_value.shape, jnp.bfloat16),
            pltpu.VMEM(w_out.shape, jnp.bfloat16),
            pltpu.VMEM((8, HEAD_DIM), jnp.float32),
            pltpu.VMEM((BLOCK, HEAD_DIM), jnp.float32),
            pltpu.VMEM((BLOCK, HEAD_DIM), jnp.float32),
            pltpu.VMEM((2, 2 * HALF, HEAD_DIM), jnp.bfloat16),
            pltpu.VMEM((128, 2 * HALF, HEAD_DIM), jnp.bfloat16),
            pltpu.VMEM((Q_PER_KV * BLOCK, HEAD_DIM), jnp.bfloat16),
            pltpu.VMEM((2, Q_PER_KV * BLOCK, HEAD_DIM), jnp.bfloat16),
            pltpu.VMEM((128, 8, HALF), jnp.float32),
            pltpu.VMEM((2, Q_PER_KV * BLOCK, HEAD_DIM), jnp.float32),
            pltpu.VMEM((2, Q_PER_KV * BLOCK, HEAD_DIM), jnp.float32),
            pltpu.VMEM((2, 2, 512, HEAD_DIM), jnp.bfloat16),
            pltpu.VMEM((2, 2, 512, HEAD_DIM), jnp.bfloat16),
            pltpu.VMEM((2, 2, 8, 512), jnp.float32),
            pltpu.VMEM((2, 2, 8, 512), jnp.float32),
            pltpu.VMEM((2, 2, 8, 512), jnp.float32),
            pltpu.VMEM((2, HALF, Q_PER_KV * HEAD_DIM), jnp.bfloat16),
            pltpu.VMEM((N_TP, ROWS, width), jnp.float32),
            pltpu.VMEM((2, N_X, ROWS // 2, width), jnp.bfloat16),
            pltpu.VMEM((2, N_X, ROWS // 2, width), jnp.bfloat16),
            pltpu.VMEM((2, N_X, ROWS // 2, width), jnp.bfloat16),
            pltpu.VMEM((2, N_X, ROWS // 2, width), jnp.bfloat16),
            dma((11,)), dma((1,)), dma((7,)), dma((2,)), dma((2, 4)), dma((1,)), dma((2, 8)),
            dma((1,)), dma((2, 10)), dma((2,)), dma((2,)), dma((2, 2)), dma((2, 2, 2)),
            dma((2,)), dma((2,)), dma((2,)), dma((2,)),
        ],
        compiler_params=pltpu.CompilerParams(
            collective_id=0, has_side_effects=True, vmem_limit_bytes=48 * 2 ** 20),
        name="fused_attention",
    )
    operands = (tokens, valid_len, norm_gain.reshape(1, -1), w_query, w_key, w_value,
                q_gain.reshape(1, -1), k_gain.reshape(1, -1), w_out, jnp.asarray(rows), jnp.asarray(cols))
    return call(*[o if o is valid_len else pltpu.with_memory_space_constraint(o, pltpu.HBM) for o in operands])


def solution(mesh):
    return jax.shard_map(
        on_device,
        mesh=mesh,
        in_specs=(
            P(("sp", "tp"), None),
            P(),
            P(),
            P(None, "tp"),
            P(None, "tp"),
            P(None, "tp"),
            P(),
            P(),
            P("tp", None),
        ),
        out_specs=P(("sp", "tp"), None),
        check_vma=False,
    )
```

```python
import functools
import math

import jax
import jax.numpy as jnp
import numpy as np
from jax import lax
from jax.experimental import pallas as pl
from jax.experimental.pallas import tpu as pltpu
from jax.sharding import PartitionSpec as P

HEAD_DIM = 128
Q_PER_KV = 4
GRID_W = 64
RING = 8
N_TP = 8
N_X = 4
ROWS = 32
BLOCK = 256
HALF = 128
EPS = 1e-06
MESH = pl.DeviceIdType.MESH
STAY = (0, 2, -2, 4)
MOVE = (1, -1, 3, -3)
SOURCE = (0, -1, -2, -3, 1, 2, 3, 4)
Q_SCALE = HEAD_DIM ** -0.5 * math.log2(math.e)


def rope_constants():
    freq = np.float32(10000.0) ** (-(np.arange(32, dtype=np.float32) * 2.0) / 64)
    freq = freq.astype(np.float32)
    sign = np.concatenate([-np.ones(32), np.ones(32)]).astype(np.float32)

    def table(count):
        angle = (np.arange(count, dtype=np.float32)[:, None] * freq[None, :]).astype(np.float64)
        angle = np.concatenate([angle, angle], axis=1)
        return np.cos(angle).astype(np.float32), np.sin(angle).astype(np.float32) * sign

    row_cos, row_sin = table(256)
    col_cos, col_sin = table(64)
    rows = np.zeros((64, 8, 128), np.float32)
    rows[:, 0:4, 0:64] = row_cos.reshape(64, 4, 64)
    rows[:, 4:8, 0:64] = row_sin.reshape(64, 4, 64)
    cols = np.zeros((2, 64, 128), np.float32)
    cols[0, :, 64:] = col_cos
    cols[1, :, 64:] = col_sin
    return rows, cols


def kernel(tok_hbm, valid_hbm, ngain_hbm, wq_hbm, wk_hbm, wv_hbm, qgain_hbm, kgain_hbm, wo_hbm, rowtab_hbm, coltab_hbm,
           out, tok, valid, ngain, qgain, kgain, coltab, x, wq, wk, wv, wo, rowtab, cosv, sinv, mine, kv, qs, q, mask, acc, lsum, o_out, o_in, l_out, l_in, den, att, partial, to_twin, from_twin, summed, arrived,
           w_sem, xs_sem, xr_sem, s1_sem, r1_sem, s2_sem, r2_sem,
           st_sem, rt_sem, qs_sem, qr_sem, gs_sem, gr_sem, ds_sem, dr_sem, os_sem, or_sem):
    sp = lax.axis_index("sp")
    tp = lax.axis_index("tp")
    z = sp // RING
    y = sp % RING

    def wrap(a):
        return lax.rem(a + 2 * RING, RING)

    core = lax.rem(tp, 2)
    column = tp // 2
    other = tp + 1 - 2 * core
    twin = {"sp": sp, "tp": other}
    peers = [{"sp": sp, "tp": lax.rem(tp + 2 * k, N_TP)} for k in range(1, N_X)]
    moves = (core != lax.rem(y, 2), core != lax.rem(z, 2))
    moved = [m.astype(jnp.int32) for m in moves]

    def at(part_id, first, second, where):
        dz, dy = (second, first) if part_id == 0 else (first, second)
        return {"sp": wrap(z + dz) * RING + wrap(y + dy), "tp": where}

    ring = [[at(a, 0, step, tp) for step in (1, -1)] for a in range(2)]
    partner = [at(0, 1 - 2 * lax.rem(y, 2), 0, other), at(1, 1 - 2 * lax.rem(z, 2), 0, other)]

    def shift(flag, k):
        return MOVE[k] * flag + STAY[k] * (1 - flag)

    def choose(a, if_moved, if_not):
        return if_moved * moved[a] + if_not * (1 - moved[a])

    two_on = [[at(a, step, 0, tp) for step in (2, -2)] for a in range(2)]
    landing = [[at(a, shift(moved[a], k), 0, choose(a, other, tp)) for k in range(3)]
               for a in range(2)]

    loads = [
        pltpu.make_async_copy(wk_hbm, wk, w_sem.at[0]),
        pltpu.make_async_copy(wv_hbm, wv, w_sem.at[1]),
        pltpu.make_async_copy(rowtab_hbm.at[sp], rowtab, w_sem.at[2]),
        pltpu.make_async_copy(wq_hbm, wq, w_sem.at[3]),
        pltpu.make_async_copy(wo_hbm, wo, w_sem.at[4]),
        pltpu.make_async_copy(coltab_hbm, coltab, w_sem.at[5]),
        pltpu.make_async_copy(qgain_hbm, qgain, w_sem.at[6]),
        pltpu.make_async_copy(kgain_hbm, kgain, w_sem.at[7]),
    ]
    early = [
        pltpu.make_async_copy(tok_hbm, tok, w_sem.at[8]),
        pltpu.make_async_copy(ngain_hbm, ngain, w_sem.at[9]),
        pltpu.make_async_copy(valid_hbm, valid, w_sem.at[10]),
    ]
    for load in early:
        load.start()
    for load in loads:
        load.start()

    barrier = pltpu.get_barrier_semaphore()
    everyone = peers + [twin] + ring[0] + ring[1] + two_on[0] + two_on[1]
    for peer in everyone:
        pl.semaphore_signal(barrier, inc=1, device_id=peer, device_id_type=MESH)
    for a in range(2):
        @pl.when(moves[a])
        def _():
            for k in range(2):
                pl.semaphore_signal(barrier, inc=1, device_id=landing[a][k], device_id_type=MESH)

    for load in early:
        load.wait()
    scaled = tok[...].astype(jnp.float32)
    inv = lax.rsqrt(jnp.mean(scaled * scaled, axis=-1, keepdims=True) + EPS)
    x[tp] = (scaled * inv * ngain[...]).astype(jnp.bfloat16)
    acc[...] = jnp.zeros_like(acc)
    lsum[...] = jnp.zeros_like(lsum)

    pl.semaphore_wait(barrier, len(everyone) + 2 * moved[0] + 2 * moved[1])

    def together(ref, send, recv):
        return pltpu.make_async_remote_copy(
            src_ref=ref, dst_ref=ref, send_sem=send, recv_sem=recv, device_id=twin, device_id_type=MESH)

    def xcopy(i):
        slot = tp if i < N_X else lax.rem(tp + 2 * N_TP - 2 * (i - N_X + 1), N_TP)
        return pltpu.make_async_remote_copy(
            src_ref=x.at[slot], dst_ref=x.at[slot], send_sem=xs_sem.at[0], recv_sem=xr_sem.at[i],
            device_id=peers[i - 1] if 0 < i < N_X else twin, device_id_type=MESH)

    for i in (2, 1, 3, 0):
        xcopy(i).start()

    for i in (2, 5, 6, 7):
        loads[i].wait()
    for r in range(4):
        cosv[r * 64:(r + 1) * 64, :] = rowtab[r:r + 1, :] + coltab[0]
        sinv[r * 64:(r + 1) * 64, :] = rowtab[4 + r:5 + r, :] + coltab[1]

    limit = valid[0]
    lane = lax.broadcasted_iota(jnp.int32, (1, HALF), 1)

    def mask_row(slot, block, half):
        pos = block * BLOCK + half * HALF + lane
        mask[slot] = jnp.broadcast_to((pos < limit).astype(jnp.float32), (8, HALF))

    for a in range(2):
        for side in range(2):
            flag = moved[a] if side == 0 else 1 - moved[a]
            for e in range(8):
                for k in range(4):
                    place = at(a, -shift(flag, k), SOURCE[e], tp)
                    mask_row(a * 64 + side * 32 + e * 4 + k, place["sp"], a)

    loads[0].wait()
    loads[1].wait()
    for k in (1, 3, 2):
        xcopy(k).wait_recv()
        xcopy(k + N_X - 1).start()
    for i in (0, 4, 6, 5):
        xcopy(i).wait_recv()

    everything = x[...].reshape(BLOCK, x.shape[2])
    cosine = cosv[...]
    sine = sinv[...]
    in_first = (lax.broadcasted_iota(jnp.int32, (BLOCK, HEAD_DIM), 1) % 64) < 32

    def turn(projected, gain, factor):
        v = projected.astype(jnp.bfloat16).astype(jnp.float32)
        u = v * lax.rsqrt(jnp.mean(v * v, axis=-1, keepdims=True) + EPS) * gain
        moved = jnp.where(in_first, pltpu.roll(u, 96, 1), pltpu.roll(u, 32, 1))
        return (u * cosine + moved * sine) * factor

    keys = turn(jnp.dot(everything, wk[...], preferred_element_type=jnp.float32), kgain[...], 1.0)
    rows = sp * BLOCK + lax.broadcasted_iota(jnp.int32, (BLOCK, HEAD_DIM), 0)
    vals = jnp.dot(everything, wv[...], preferred_element_type=jnp.float32)
    vals = jnp.where(rows < limit, vals, 0.0).astype(jnp.bfloat16)
    for a in range(2):
        piece = slice(a * HALF, (a + 1) * HALF)
        mine[a, 0:HALF, :] = keys[piece, :].T.astype(jnp.bfloat16)
        mine[a, HALF:, :] = vals[piece, :]

    def spread(a, k, h):
        return pltpu.make_async_remote_copy(
            src_ref=mine.at[a, pl.ds(h * HALF, HALF)], dst_ref=kv.at[a * 64 + k, pl.ds(h * HALF, HALF)],
            send_sem=s1_sem.at[a], recv_sem=r1_sem.at[a, k, h],
            device_id=landing[a][k], device_id_type=MESH)

    def pass_up(a, h):
        return pltpu.make_async_remote_copy(
            src_ref=kv.at[a * 64, pl.ds(h * HALF, HALF)], dst_ref=kv.at[a * 64 + 2, pl.ds(h * HALF, HALF)],
            send_sem=s1_sem.at[a], recv_sem=r1_sem.at[a, 2, h],
            device_id=two_on[a][0], device_id_type=MESH)

    def pass_on(a, h):
        odd = lax.rem((y if a == 0 else z) // 2, 2)
        upwards = odd * (1 - moved[a])
        return pltpu.make_async_remote_copy(
            src_ref=kv.at[a * 64 + choose(a, 1, 2 - odd), pl.ds(h * HALF, HALF)],
            dst_ref=kv.at[a * 64 + 3, pl.ds(h * HALF, HALF)], send_sem=s1_sem.at[a], recv_sem=r1_sem.at[a, 3, h], device_id=at(a, 4 * upwards - 2, 0, tp), device_id_type=MESH)

    def slot(a, side, e, p):
        return a * 64 + side * 32 + e * 4 + 2 * p

    def hop(a, d, p, e_from, e_to, i):
        return pltpu.make_async_remote_copy(
            src_ref=kv.at[pl.ds(slot(a, 0, e_from, p), 2)], dst_ref=kv.at[pl.ds(slot(a, 0, e_to, p), 2)],
            send_sem=s2_sem.at[0], recv_sem=r2_sem.at[a, i + d if isinstance(i, int) and i == 6 else i],
            device_id=ring[a][d], device_id_type=MESH)

    def share(a, e, p, i):
        return pltpu.make_async_remote_copy(
            src_ref=kv.at[pl.ds(slot(a, 0, e, p), 2)], dst_ref=kv.at[pl.ds(slot(a, 1, e, p), 2)],
            send_sem=st_sem.at[0], recv_sem=rt_sem.at[a, i],
            device_id=twin, device_id_type=MESH)

    for h in range(2):
        for a in range(2):
            spread(a, 1, h).start()

            @pl.when(moves[a])
            def _():
                spread(a, 0, h).start()

            @pl.when(jnp.logical_not(moves[a]))
            def _():
                spread(a, 2, h).start()
                kv[a * 64, h * HALF:(h + 1) * HALF, :] = mine[a, h * HALF:(h + 1) * HALF, :]

    loads[3].wait()
    for h in range(Q_PER_KV):
        query = jnp.dot(everything, wq[:, h * HEAD_DIM:(h + 1) * HEAD_DIM], preferred_element_type=jnp.float32)
        query = turn(query, qgain[...], Q_SCALE).astype(jnp.bfloat16)
        query = query.reshape(N_TP, 2, ROWS // 2, HEAD_DIM)
        for r in range(2):
            qs[r * 512 + h * HALF:r * 512 + (h + 1) * HALF, :] = query[:, r].reshape(HALF, HEAD_DIM)

    def swap_query(a):
        return pltpu.make_async_remote_copy(
            src_ref=qs, dst_ref=q.at[a], send_sem=qs_sem.at[a], recv_sem=qr_sem.at[a],
            device_id=partner[a], device_id_type=MESH)

    for a in range(2):
        @pl.when(moves[a])
        def _():
            swap_query(a).start()

        @pl.when(jnp.logical_not(moves[a]))
        def _():
            q[a] = qs[...]

    def attend(a, slots, rows):
        kt = jnp.concatenate([kv[s, 0:HALF, :] for s in slots], axis=1)
        v = jnp.concatenate([kv[s, HALF:, :] for s in slots], axis=0)
        marks = [mask[s, 0:1, :] for s in slots]
        for r in rows:
            span = pl.ds(r * 512, 512)
            s = jnp.dot(q[a, span, :], kt, preferred_element_type=jnp.float32)
            w = jnp.exp2(s)
            acc[a, span, :] += jnp.dot(w.astype(jnp.bfloat16), v, preferred_element_type=jnp.float32)
            t = w[:, 0:HALF] * marks[0]
            for i in range(1, len(slots)):
                t = t + w[:, i * HALF:(i + 1) * HALF] * marks[i]
            lsum[a, span, :] += t

    def hand_on(a, p):
        for d in range(2):
            hop(a, d, p, 0, 3 * d + 1, p).start()
        share(a, 0, p, p).start()

    for h in range(2):
        for a in range(2):
            @pl.when(moves[a])
            def _():
                spread(a, 0, h).wait_recv()
                pass_up(a, h).start()
            spread(a, 1, h).wait_recv()

            @pl.when(jnp.logical_not(moves[a]))
            def _():
                spread(a, 2, h).wait_recv()
            pass_on(a, h).start()
    for a in range(2):
        hand_on(a, 0)

    for a in range(2):
        @pl.when(moves[a])
        def _():
            swap_query(a).wait_recv()

    def own(a, p):
        share(a, 0, p, p).wait_recv()
        attend(a, [slot(a, side, 0, p) + i for side in range(2) for i in range(2)], (0, 1))

    for a in range(2):
        own(a, 0)
    for a in range(2):
        @pl.when(moves[a])
        def _():
            for h in range(2):
                pass_up(a, h).wait_recv()
        for h in range(2):
            pass_on(a, h).wait_recv()
        hand_on(a, 1)

    def receive(i):
        e, p = i // 2 + 1, lax.rem(i, 2)
        for a in range(2):
            together(kv.at[pl.ds(a * 64, 4)], s2_sem.at[0], r2_sem.at[a, i]).wait_recv()
            for d in range(2):
                @pl.when(i < 4)
                def _():
                    hop(a, d, p, 3 * d + e, 3 * d + e + 1, i + 2).start()

                @pl.when(i == 4 + d)
                def _():
                    hop(a, d, d, 3 * d + 3, 7, 6).start()
                share(a, 3 * d + e, p, i + 2).start()

    def receive_last(d):
        for a in range(2):
            hop(a, d, d, 0, 7, 6).wait_recv()
            share(a, 7, d, 8 + d).start()

    def use(a, i):
        e, p = i // 2 + 1, lax.rem(i, 2)
        together(kv.at[pl.ds(a * 64, 4)], st_sem.at[0], rt_sem.at[a, i + 2]).wait_recv()
        attend(a, [slot(a, side, 3 * d + e, p) + n for side in range(2) for d in range(2) for n in range(2)], (0, 1))

    own(0, 1)
    receive(jnp.int32(0))
    own(1, 1)

    def stage(i, c):
        use(0, i)

        @pl.when(i < 5)
        def _():
            receive(i + 1)

        @pl.when(i == 5)
        def _():
            receive_last(0)
        use(1, i)
        return c

    lax.fori_loop(0, 6, stage, 0)

    def final_slots(a, p):
        share(a, 7, p, 8 + p).wait_recv()
        return [slot(a, side, 7, p) + i for side in range(2) for i in range(2)]

    attend(0, final_slots(0, 0), (0, 1))
    receive_last(1)
    attend(1, final_slots(1, 0), (0, 1))

    def give_back(a, r):
        return (
            pltpu.make_async_remote_copy(
                src_ref=o_out.at[a, r], dst_ref=o_in.at[a, r], send_sem=gs_sem.at[a, 0],
                recv_sem=gr_sem.at[a, r, 0], device_id=partner[a], device_id_type=MESH),
            pltpu.make_async_remote_copy(
                src_ref=l_out.at[a, r], dst_ref=l_in.at[a, r], send_sem=gs_sem.at[a, 1],
                recv_sem=gr_sem.at[a, r, 1], device_id=partner[a], device_id_type=MESH),
        )

    ones = jnp.ones((8, HALF), jnp.bfloat16)

    def finish(a, r):
        span = slice(r * 512, (r + 1) * 512)
        @pl.when(moves[a])
        def _():
            o_out[a, r] = acc[a, span, :].astype(jnp.bfloat16)
            give_back(a, r)[0].start()

        sums = lsum[a, span, :]
        high = sums.astype(jnp.bfloat16)
        low = (sums - high.astype(jnp.float32)).astype(jnp.bfloat16)
        across = (((1,), (1,)), ((), ()))
        l_out[a, r] = (lax.dot_general(ones, high, across, preferred_element_type=jnp.float32)
                       + lax.dot_general(ones, low, across, preferred_element_type=jnp.float32))

        @pl.when(moves[a])
        def _():
            give_back(a, r)[1].start()

    def gather_back(r):
        span = slice(r * 512, (r + 1) * 512)
        for a in range(2):
            @pl.when(moves[a])
            def _():
                for copy in give_back(a, r):
                    copy.wait_recv()
                acc[a, span, :] = o_in[a, r].astype(jnp.float32)
                den[a, r] = l_in[a, r]

            @pl.when(jnp.logical_not(moves[a]))
            def _():
                den[a, r] = l_out[a, r]

    def project_out(r):
        totals = (den[0, r] + den[1, r]).T
        for h in range(Q_PER_KV):
            span = slice(r * 512 + h * HALF, r * 512 + (h + 1) * HALF)
            rows_of = slice(h * HALF, (h + 1) * HALF)
            att[r, :, h * HEAD_DIM:(h + 1) * HEAD_DIM] = (
                (acc[0, span, :] + acc[1, span, :]) / totals[rows_of, 0:1]).astype(jnp.bfloat16)
        mixed = jnp.dot(att[r], wo[...], preferred_element_type=jnp.float32)
        part_rows = slice(r * ROWS // 2, (r + 1) * ROWS // 2)
        partial[:, part_rows, :] = mixed.reshape(N_TP, ROWS // 2, mixed.shape[1])
        for i in range(N_X):
            to_twin[r, i] = partial[2 * i + 1 - core, part_rows, :].astype(jnp.bfloat16)
        pair(r).start()

    def pair(r):
        return pltpu.make_async_remote_copy(
            src_ref=to_twin.at[r], dst_ref=from_twin.at[r], send_sem=ds_sem.at[r], recv_sem=dr_sem.at[r],
            device_id=twin, device_id_type=MESH)

    def along(r, i):
        return pltpu.make_async_remote_copy(
            src_ref=summed.at[r, i], dst_ref=arrived.at[r, column], send_sem=os_sem.at[r],
            recv_sem=or_sem.at[r], device_id={"sp": sp, "tp": 2 * i + core}, device_id_type=MESH)

    def add_pair(r):
        pair(r).wait_recv()
        part_rows = slice(r * ROWS // 2, (r + 1) * ROWS // 2)
        for i in range(N_X):
            both_cores = partial[2 * i + core, part_rows, :] + from_twin[r, i].astype(jnp.float32)
            partial[2 * i + core, part_rows, :] = both_cores
            summed[r, i] = both_cores.astype(jnp.bfloat16)

            @pl.when(column != i)
            def _():
                along(r, i).start()

    slots = [final_slots(a, 1) for a in range(2)]
    for r in range(2):
        for a in range(2):
            attend(a, slots[a], (r,))
        for a in range(2):
            finish(a, r)

    loads[4].wait()
    together(x.at[pl.ds(0, 2 * N_X - 1)], xs_sem.at[0], xr_sem.at[0]).wait_send()
    for a in range(2):
        @pl.when(moves[a])
        def _():
            together(kv.at[pl.ds(0, 4)], s1_sem.at[a], r1_sem.at[a, 0, 0]).wait_send()
            swap_query(a).wait_send()

        @pl.when(jnp.logical_not(moves[a]))
        def _():
            together(kv.at[pl.ds(0, 3)], s1_sem.at[a], r1_sem.at[a, 0, 0]).wait_send()
    together(kv.at[pl.ds(0, 56)], s2_sem.at[0], r2_sem.at[0, 0]).wait_send()
    together(kv.at[pl.ds(0, 64)], st_sem.at[0], rt_sem.at[0, 0]).wait_send()

    gather_back(0)
    project_out(0)
    gather_back(1)
    add_pair(0)
    project_out(1)
    add_pair(1)
    for r in range(2):
        part_rows = slice(r * ROWS // 2, (r + 1) * ROWS // 2)
        total = partial[tp, part_rows, :]
        together(arrived.at[r, pl.ds(0, N_X - 1)], os_sem.at[r], or_sem.at[r]).wait_recv()
        for k in range(1, N_X):
            total = total + arrived[r, lax.rem(column + N_X - k, N_X)].astype(jnp.float32)
        out[part_rows, :] = total.astype(jnp.bfloat16)
    for a in range(2):
        @pl.when(moves[a])
        def _():
            together(o_out.at[a], gs_sem.at[a, 0], gr_sem.at[a, 0, 0]).wait_send()
            together(l_out.at[a], gs_sem.at[a, 1], gr_sem.at[a, 0, 1]).wait_send()
    for r in range(2):
        pair(r).wait_send()
        together(summed.at[r, pl.ds(0, N_X - 1)], os_sem.at[r], or_sem.at[r]).wait_send()


def on_device(tokens, valid_len, norm_gain, w_query, w_key, w_value, q_gain, k_gain, w_out):
    rows, cols = rope_constants()
    width = tokens.shape[1]
    vmem = pl.BlockSpec(memory_space=pltpu.VMEM)
    anywhere = pl.BlockSpec(memory_space=pltpu.HBM)
    dma = pltpu.SemaphoreType.DMA
    call = pl.pallas_call(
        kernel,
        out_shape=jax.ShapeDtypeStruct(tokens.shape, jnp.bfloat16),
        in_specs=[anywhere] * 11,
        out_specs=vmem,
        scratch_shapes=[
            pltpu.VMEM(tokens.shape, jnp.bfloat16),
            pltpu.SMEM((1,), jnp.int32),
            pltpu.VMEM((1, width), jnp.float32),
            pltpu.VMEM((1, HEAD_DIM), jnp.float32),
            pltpu.VMEM((1, HEAD_DIM), jnp.float32),
            pltpu.VMEM(cols.shape, jnp.float32),
            pltpu.VMEM((N_TP, ROWS, width), jnp.bfloat16),
            pltpu.VMEM(w_query.shape, jnp.bfloat16),
            pltpu.VMEM(w_key.shape, jnp.bfloat16),
            pltpu.VMEM(w_value.shape, jnp.bfloat16),
            pltpu.VMEM(w_out.shape, jnp.bfloat16),
            pltpu.VMEM((8, HEAD_DIM), jnp.float32),
            pltpu.VMEM((BLOCK, HEAD_DIM), jnp.float32),
            pltpu.VMEM((BLOCK, HEAD_DIM), jnp.float32),
            pltpu.VMEM((2, 2 * HALF, HEAD_DIM), jnp.bfloat16),
            pltpu.VMEM((128, 2 * HALF, HEAD_DIM), jnp.bfloat16),
            pltpu.VMEM((Q_PER_KV * BLOCK, HEAD_DIM), jnp.bfloat16),
            pltpu.VMEM((2, Q_PER_KV * BLOCK, HEAD_DIM), jnp.bfloat16),
            pltpu.VMEM((128, 8, HALF), jnp.float32),
            pltpu.VMEM((2, Q_PER_KV * BLOCK, HEAD_DIM), jnp.float32),
            pltpu.VMEM((2, Q_PER_KV * BLOCK, HEAD_DIM), jnp.float32),
            pltpu.VMEM((2, 2, 512, HEAD_DIM), jnp.bfloat16),
            pltpu.VMEM((2, 2, 512, HEAD_DIM), jnp.bfloat16),
            pltpu.VMEM((2, 2, 8, 512), jnp.float32),
            pltpu.VMEM((2, 2, 8, 512), jnp.float32),
            pltpu.VMEM((2, 2, 8, 512), jnp.float32),
            pltpu.VMEM((2, HALF, Q_PER_KV * HEAD_DIM), jnp.bfloat16),
            pltpu.VMEM((N_TP, ROWS, width), jnp.float32),
            pltpu.VMEM((2, N_X, ROWS // 2, width), jnp.bfloat16),
            pltpu.VMEM((2, N_X, ROWS // 2, width), jnp.bfloat16),
            pltpu.VMEM((2, N_X, ROWS // 2, width), jnp.bfloat16),
            pltpu.VMEM((2, N_X, ROWS // 2, width), jnp.bfloat16),
            dma((11,)), dma((1,)), dma((7,)), dma((2,)), dma((2, 4, 2)), dma((1,)), dma((2, 8)),
            dma((1,)), dma((2, 10)), dma((2,)), dma((2,)), dma((2, 2)), dma((2, 2, 2)),
            dma((2,)), dma((2,)), dma((2,)), dma((2,)),
        ],
        compiler_params=pltpu.CompilerParams(
            collective_id=0, has_side_effects=True, vmem_limit_bytes=48 * 2 ** 20),
        name="fused_attention",
    )
    operands = (tokens, valid_len, norm_gain.reshape(1, -1), w_query, w_key, w_value,
                q_gain.reshape(1, -1), k_gain.reshape(1, -1), w_out, jnp.asarray(rows), jnp.asarray(cols))
    return call(*[o if o is valid_len else pltpu.with_memory_space_constraint(o, pltpu.HBM) for o in operands])


def solution(mesh):
    return jax.shard_map(
        on_device,
        mesh=mesh,
        in_specs=(
            P(("sp", "tp"), None),
            P(),
            P(),
            P(None, "tp"),
            P(None, "tp"),
            P(None, "tp"),
            P(),
            P(),
            P("tp", None),
        ),
        out_specs=P(("sp", "tp"), None),
        check_vma=False,
    )
```
